256 devices in a mesh: ep: 16 (over y, x), tp: 16 (over z, core).
Axes of the slice: x: 4, y: 4, z: 8, core: 2. Of those that a mesh axis runs over, the one named last changes fastest.
Arguments:
- tokens: bfloat16 [512, 4096], P('ep'), may hold values from -6 to 6
- state_matrix: float32 [512, 16, 128, 128], P('ep', 'tp'), may hold values from -1.5 to 1.5
- state_norm: float32 [512, 16, 128], P('ep', 'tp'), may hold values from -4 to 4
- state_max: float32 [512, 16], P('ep', 'tp'), may hold values from -5 to 5
- mixer_gain: float32 [4096], replicated, may hold values from 0.1 to 1.9
- w_query: bfloat16 [4096, 2048], P('ep', 'tp'), may hold values from -0.09375 to 0.09375
- w_key: bfloat16 [4096, 2048], P('ep', 'tp'), may hold values from -0.09375 to 0.09375
- w_value: bfloat16 [4096, 2048], P('ep', 'tp'), may hold values from -0.09375 to 0.09375
- w_outgate: bfloat16 [4096, 2048], P('ep', 'tp'), may hold values from -0.09375 to 0.09375
- w_ingate: bfloat16 [4096, 16], replicated, may hold values from -0.09375 to 0.09375
- w_forget: bfloat16 [4096, 16], replicated, may hold values from -0.09375 to 0.09375
- forget_bias: float32 [16], replicated, may hold values from -2 to 4
- w_proj: bfloat16 [2048, 4096], P('tp', 'ep'), may hold values from -0.125 to 0.125
- ffn_gain: float32 [4096], replicated, may hold values from 0.1 to 1.9
- w_branch: bfloat16 [4096], replicated, may hold values from -0.09375 to 0.09375
- routes: int32 [512, 2], P('ep'), may hold values from 0 to 15, all different within a row; in each aligned block of 32 rows (0 to 31, 32 to 63, ...) at most 6 rows name the same one
- route_weight: float32 [512, 2], P('ep'), may hold values from 0.2 to 1
- expert_gate: bfloat16 [16, 4096, 4096], P('ep', None, 'tp'), may hold values from -0.09375 to 0.09375
- expert_up: bfloat16 [16, 4096, 4096], P('ep', None, 'tp'), may hold values from -0.09375 to 0.09375
- expert_down: bfloat16 [16, 4096, 4096], P('ep', 'tp'), may hold values from -0.09375 to 0.09375
- dense_gate: bfloat16 [4096, 8192], P('ep', 'tp'), may hold values from -0.09375 to 0.09375
- dense_up: bfloat16 [4096, 8192], P('ep', 'tp'), may hold values from -0.09375 to 0.09375
- dense_down: bfloat16 [8192, 4096], P('tp', 'ep'), may hold values from -0.0625 to 0.0625
Outputs:
- layer_out: bfloat16 [512, 4096], P('ep')
- new_matrix: float32 [512, 16, 128, 128], P('ep', 'tp')
- new_norm: float32 [512, 16, 128], P('ep', 'tp')
- new_max: float32 [512, 16], P('ep', 'tp')
The draws below stay inside these ranges and needn't reach their ends.
Inputs may be any that keep to these rules, and one draw needn't show every extreme that they name: `routes`: each row names 2 different experts. Among the rows of one index of ep (32 sequences) no expert is named more than 6 times, and in some such group one expert is named exactly 6 times.
All inputs are finite; a program needn't handle non-finite values.
Results may differ from the reference program's by a relative error of at most 0.012.
Values may be sent and summed in bfloat16 or wider, within the bound.
A program may use at most 64 MiB of HBM per device.

```python
import math
import jax
import jax.numpy as jnp
import numpy as np
from jax import lax

D = 4096
HEADS = 16
HDIM = 128
MW = 2048
FFD = 8192
FFE = 4096
TOPK = 2
SEQS = 32
BATCH = 512
EXPERTS = 16
CAP = 6
N_EP = 16


def shard_levels(stream_key, shape, pieces, low, high):
    def one(axis_at, parts):
        draws = jax.random.uniform(jax.random.fold_in(jax.random.fold_in(stream_key, 6), axis_at), (parts,), jnp.float32, low / len(pieces), high / len(pieces))
        return jnp.repeat(jnp.exp(draws), shape[axis_at] // parts).reshape((-1,) + (1,) * (len(shape) - axis_at - 1))

    level = one(*pieces[0])
    for cut in pieces[1:]:
        level = level * one(*cut)
    return level


def shared_out(key, own, number, rows, amount, top, limit, slope):
    ranking = jax.random.permutation(key, amount)
    crowded, usual = load_shares(amount, rows * top, limit, slope, True), load_shares(amount, rows * top, limit, slope, False)
    places = jnp.arange(amount)

    def named(lengths, turn):
        used = int((lengths > 0).sum())
        fixed = max(1, used // 4)
        shifted = fixed + (places - fixed + turn * (used - fixed)) % max(1, amount - fixed)
        return jnp.zeros((amount,), jnp.int32).at[ranking[jnp.where(places < fixed, places, shifted)]].set(jnp.asarray(lengths, jnp.int32))

    lengths = jnp.where(number % 4 == 0, named(crowded, number // 4), named(usual, number - number // 4 - 1))
    mixed = jax.random.permutation(jax.random.fold_in(own, 3), amount)
    giver, receiver = mixed[0:amount // 2 * 2:2], mixed[1:amount // 2 * 2:2]
    slack = jnp.minimum(lengths[giver] - 1, limit - lengths[receiver]) // 2
    slack = jnp.where((giver == ranking[0]) | (receiver == ranking[0]) | (lengths[receiver] == 0), 0, jnp.maximum(slack, 0))
    shifted = jax.random.randint(jax.random.fold_in(own, 4), (amount // 2,), 0, 1 << 20) % (slack + 1)
    lengths = lengths.at[giver].add(-shifted).at[receiver].add(shifted)
    members = jnp.searchsorted(jnp.cumsum(lengths), jnp.arange(rows * top), side="right").astype(jnp.int32)
    grid = members.reshape(top, rows).T
    grid = grid[jax.random.permutation(jax.random.fold_in(own, 1), rows)]
    turn = jax.random.randint(jax.random.fold_in(own, 2), (rows, 1), 0, top)
    return jnp.take_along_axis(grid, (jnp.arange(top)[None, :] + turn) % top, axis=1)


def load_shares(number_of, total, limit, lean, full):
    portions = [(1 << 20) // math.isqrt(standing ** lean) + 1 for standing in range(1, number_of + 1)]
    largest = limit if full else min(limit, max(-(-total // number_of), total * portions[0] // sum(portions)))
    least = 1 if total - largest >= number_of - 1 else 0
    given, surplus = [largest] + [least] * (number_of - 1), total - largest - least * (number_of - 1)
    while surplus > 0:
        movable = [i for i in range(1, number_of) if given[i] < largest] or [i for i in range(1, number_of) if given[i] < limit]
        pool, left = sum([portions[i] for i in movable]), surplus
        for i in movable:
            addition = min(limit - given[i], max(1, left * portions[i] // pool), surplus)
            given[i] = given[i] + addition
            surplus = surplus - addition
    return np.array(given)


def bell_draw(stream_key, extent, spread, reach, pieces=(), held_as=jnp.bfloat16):
    result = spread * jax.random.normal(stream_key, extent, jnp.float32)
    if pieces:
        result = result * shard_levels(stream_key, extent, pieces, -0.22, 0.18)
    return jnp.clip(result, -reach, reach).astype(held_as)


def setup_inputs(seed: int = 0) -> dict:
    key_of = jax.random.split(jax.random.key(seed), 24)
    tokens = bell_draw(key_of[0], (BATCH, D), 1.0, 6.0, ((0, 16),))
    state_matrix = bell_draw(key_of[1], (BATCH, HEADS, HDIM, HDIM), 0.1, 1.5, ((0, 16), (1, 16)), jnp.float32)
    state_norm = bell_draw(key_of[2], (BATCH, HEADS, HDIM), 0.3, 4.0, ((0, 16), (1, 16)), jnp.float32)
    state_max = bell_draw(key_of[3], (BATCH, HEADS), 1.0, 5.0, ((0, 16), (1, 16)), jnp.float32)
    mixer_gain = jnp.clip(1.0 + 0.18 * jax.random.normal(key_of[4], (D,), jnp.float32), 0.1, 1.9)
    w_query = bell_draw(key_of[5], (D, MW), D ** -0.5, 0.09375, ((0, 16), (1, 16)))
    w_key = bell_draw(key_of[6], (D, MW), D ** -0.5, 0.09375, ((0, 16), (1, 16)))
    w_value = bell_draw(key_of[7], (D, MW), D ** -0.5, 0.09375, ((0, 16), (1, 16)))
    w_outgate = bell_draw(key_of[8], (D, MW), D ** -0.5, 0.09375, ((0, 16), (1, 16)))
    w_ingate = bell_draw(key_of[9], (D, HEADS), D ** -0.5, 0.09375)
    w_forget = bell_draw(key_of[10], (D, HEADS), D ** -0.5, 0.09375)
    forget_bias = jnp.clip(jax.random.uniform(key_of[11], (HEADS,), jnp.float32, -2.0, 4.0), -2.0, 4.0)
    w_proj = bell_draw(key_of[12], (MW, D), MW ** -0.5, 0.125, ((0, 16), (1, 16)))
    ffn_gain = jnp.clip(1.0 + 0.18 * jax.random.normal(key_of[13], (D,), jnp.float32), 0.1, 1.9)
    w_branch = bell_draw(key_of[14], (D,), D ** -0.5, 0.09375)
    routes_keys = jax.random.split(jax.random.fold_in(key_of[15], 1), BATCH // SEQS)
    routes_turns = jax.random.permutation(jax.random.fold_in(key_of[15], 3), BATCH // SEQS)
    routes = jax.vmap(lambda own, number: shared_out(jax.random.fold_in(key_of[15], 2), own, number, SEQS, EXPERTS, TOPK, CAP, 2))(routes_keys, routes_turns).reshape((BATCH, TOPK))
    route_weight = jnp.clip(jnp.exp(math.log(1.0) - 1.609438 * jax.random.uniform(key_of[16], (BATCH, TOPK), jnp.float32) ** shard_levels(key_of[16], (BATCH, TOPK), ((0, 16),), -0.2, 0.2)), 0.2, 1.0)
    expert_gate = bell_draw(key_of[17], (EXPERTS, D, FFE), D ** -0.5, 0.09375, ((0, 16), (2, 16)))
    expert_up = bell_draw(key_of[18], (EXPERTS, D, FFE), D ** -0.5, 0.09375, ((0, 16), (2, 16)))
    expert_down = bell_draw(key_of[19], (EXPERTS, FFE, D), FFE ** -0.5, 0.09375, ((0, 16), (1, 16)))
    dense_gate = bell_draw(key_of[20], (D, FFD), D ** -0.5, 0.09375, ((0, 16), (1, 16)))
    dense_up = bell_draw(key_of[21], (D, FFD), D ** -0.5, 0.09375, ((0, 16), (1, 16)))
    dense_down = bell_draw(key_of[22], (FFD, D), FFD ** -0.5, 0.0625, ((0, 16), (1, 16)))
    return dict(tokens=tokens, state_matrix=state_matrix, state_norm=state_norm, state_max=state_max, mixer_gain=mixer_gain, w_query=w_query, w_key=w_key, w_value=w_value, w_outgate=w_outgate, w_ingate=w_ingate, w_forget=w_forget, forget_bias=forget_bias, w_proj=w_proj, ffn_gain=ffn_gain, w_branch=w_branch, routes=routes, route_weight=route_weight, expert_gate=expert_gate, expert_up=expert_up, expert_down=expert_down, dense_gate=dense_gate, dense_up=dense_up, dense_down=dense_down)


EPS = 1e-06

def rms_scale(values, gain):
    wide = values.astype(jnp.float32)
    return wide * lax.rsqrt(lax.optimization_barrier(jnp.mean(wide * wide, axis=-1, keepdims=True)) + EPS) * gain.astype(jnp.float32)

def slot_numbers(flat_routes, experts_all):
    onehot = (flat_routes[:, None] == jnp.arange(experts_all, dtype=jnp.int32)[None, :]).astype(jnp.int32)
    before = jnp.cumsum(onehot, axis=0) - onehot
    return lax.optimization_barrier(jnp.sum(before * onehot, axis=1)).astype(jnp.int32)

def memory_step(query_all, key_all, value_all, outgate, gate_in, gate_forget, state_matrix, state_norm, state_max):
    row_count, head_count = gate_in.shape
    head_size = state_matrix.shape[-1]
    heads_q = query_all.reshape(row_count, head_count, head_size)
    heads_k = key_all.reshape(row_count, head_count, head_size) * head_size ** (-0.5)
    heads_v = value_all.reshape(row_count, head_count, head_size)
    log_keep = jax.nn.log_sigmoid(gate_forget)
    new_max = jnp.maximum(log_keep + state_max, gate_in)
    keep_factor = jnp.exp(log_keep + state_max - new_max)
    write_factor = jnp.exp(gate_in - new_max)
    new_matrix = keep_factor[:, :, None, None] * state_matrix + write_factor[:, :, None, None] * heads_k[:, :, :, None] * heads_v[:, :, None, :]
    new_norm = keep_factor[:, :, None] * state_norm + write_factor[:, :, None] * heads_k
    numer = jnp.einsum('bhk,bhkv->bhv', heads_q, new_matrix, precision=lax.Precision.HIGHEST)
    denom = lax.optimization_barrier(jnp.sum(heads_q * new_norm, axis=-1))
    cell = numer / jnp.maximum(jnp.abs(denom), 1.0)[:, :, None]
    gated = jax.nn.sigmoid(outgate.reshape(row_count, head_count, head_size)) * cell
    mixed_heads = gated.reshape(row_count, head_count * head_size).astype(jnp.bfloat16)
    return (mixed_heads, new_matrix, new_norm, new_max)

def reference(tokens, state_matrix, state_norm, state_max, mixer_gain, w_query, w_key, w_value, w_outgate, w_ingate, w_forget, forget_bias, w_proj, ffn_gain, w_branch, routes, route_weight, expert_gate, expert_up, expert_down, dense_gate, dense_up, dense_down):
    normed = rms_scale(tokens, mixer_gain).astype(jnp.bfloat16)
    query_all = jnp.dot(normed, w_query, preferred_element_type=jnp.float32)
    key_all = jnp.dot(normed, w_key, preferred_element_type=jnp.float32)
    value_all = jnp.dot(normed, w_value, preferred_element_type=jnp.float32)
    outgate = jnp.dot(normed, w_outgate, preferred_element_type=jnp.float32)
    gate_in = jnp.dot(normed, w_ingate, preferred_element_type=jnp.float32)
    gate_forget = jnp.dot(normed, w_forget, preferred_element_type=jnp.float32) + forget_bias
    mixed_heads, new_matrix, new_norm, new_max = memory_step(query_all, key_all, value_all, outgate, gate_in, gate_forget, state_matrix, state_norm, state_max)
    mixer_out = jnp.dot(mixed_heads, w_proj, preferred_element_type=jnp.float32)
    residual = (tokens.astype(jnp.float32) + mixer_out).astype(jnp.bfloat16)
    ffn_in = rms_scale(residual, ffn_gain).astype(jnp.bfloat16)
    branch_share = jax.nn.sigmoid(jnp.dot(ffn_in, w_branch, preferred_element_type=jnp.float32))
    dense_hidden = (jax.nn.silu(jnp.dot(ffn_in, dense_gate, preferred_element_type=jnp.float32)) * jnp.dot(ffn_in, dense_up, preferred_element_type=jnp.float32)).astype(jnp.bfloat16)
    dense_out = jnp.dot(dense_hidden, dense_down, preferred_element_type=jnp.float32)
    group_routes = routes.reshape(N_EP, SEQS * TOPK)
    slots = jax.vmap(lambda group_row: slot_numbers(group_row, EXPERTS))(group_routes)
    group_ids = jnp.broadcast_to(jnp.arange(N_EP, dtype=jnp.int32)[:, None], group_routes.shape)
    repeated = jnp.repeat(ffn_in, TOPK, axis=0).reshape(N_EP, SEQS * TOPK, D)
    buffers = jnp.zeros((EXPERTS, N_EP, CAP, D), jnp.bfloat16).at[group_routes, group_ids, slots].set(repeated)

    def one_expert(index):
        rows_in = buffers[index].reshape(N_EP * CAP, D)
        hidden = (jax.nn.silu(jnp.dot(rows_in, expert_gate[index], preferred_element_type=jnp.float32)) * jnp.dot(rows_in, expert_up[index], preferred_element_type=jnp.float32)).astype(jnp.bfloat16)
        return jnp.dot(hidden, expert_down[index], preferred_element_type=jnp.float32).reshape(N_EP, CAP, D)
    results = lax.map(one_expert, jnp.arange(EXPERTS, dtype=jnp.int32))
    picked = results[group_routes, group_ids, slots].reshape(N_EP * SEQS, TOPK, D)
    shares = route_weight / lax.optimization_barrier(jnp.sum(route_weight, axis=1, keepdims=True))
    expert_rows = lax.optimization_barrier(jnp.sum(shares[:, :, None] * picked, axis=1))
    total_ffn = expert_rows + branch_share[:, None] * dense_out
    layer_out = (residual.astype(jnp.float32) + total_ffn).astype(jnp.bfloat16)
    return (layer_out, new_matrix, new_norm, new_max)
```

```python
import functools

import jax
import jax.numpy as jnp
from jax import lax
from jax.experimental import pallas as pl
from jax.experimental.pallas import tpu as pltpu
from jax.sharding import PartitionSpec as P

EPS = 1e-06
MESH = pl.DeviceIdType.MESH
F32 = jnp.float32
BF16 = jnp.bfloat16
N = 16
NZ = 8
ROWS = 32
D = 4096
COLS = 256
HALF = 2048
HD = 128


def dot(a, b):
    return jnp.dot(a, b, preferred_element_type=F32)


def dot_rows(a, b):
    return lax.dot_general(a, b, (((1,), (1,)), ((), ())), preferred_element_type=F32)


def layer_kernel(
    tok_h, st_h, sn_h, smax_h, gmix_h, wq_h, wk_h, wv_h, wo_h, wi_h, wf_h, fb_h, wp_h, gffn_h, wbr_h,
    rt_h, rw_h, eg_h, eu_h, ed_h, dg_h, du_h, dd_h,
    out_h, nm_h, nn_h, nmax_h,
    tok, st, sn, smax, gmix, wq, wi, wf, fb, wp, gffn, wbr, rt, rw, eg, eu, ed, dgu, dd,
    xall, csend, crecv, mhall, num,
    part, pd2d, rsend, rrecv, resall,
    part2, pd2d2, rsend2, rrecv2,
    rtsend, rtall, dsend, drecv, stsend, strecv, hall, r2all, aall,
    xs, xfull, aexp, acc, yp, yd2d, ys, yrecv, yout, ycomb, outv, nnv, nmaxv,
    load_sem, ssem, bsem, rsem, zsem, z2sem, store_sem,
):
    e = lax.axis_index("ep")
    t = lax.axis_index("tp")
    z = t // 2
    c = lax.rem(t, 2)
    mate = 2 * z + 1 - c

    def rcopy(src, dst, send, recv, pe, pt):
        return pltpu.make_async_remote_copy(
            src_ref=src, dst_ref=dst, send_sem=send, recv_sem=recv, device_id=(pe, pt), device_id_type=MESH
        )

    def wait_for(ref, sem):
        pltpu.make_async_copy(ref, ref, sem).wait()

    def either(less, ref_less, ref_all, sem):
        @pl.when(less)
        def _():
            wait_for(ref_less, sem)

        @pl.when(jnp.logical_not(less))
        def _():
            wait_for(ref_all, sem)

    def up(d):
        return lax.rem(e + d, N)

    def down(d):
        return lax.rem(e + N - d, N)

    def over_ep(fn):
        lax.fori_loop(1, N, lambda d, carry: (fn(up(d)), carry)[1], 0)

    def over_z(fn):
        lax.fori_loop(1, NZ, lambda d, carry: (fn(lax.rem(z + d, NZ)), carry)[1], 0)

    def cols(index):
        return pl.ds(pl.multiple_of(index * COLS, COLS), COLS)

    def half(index):
        return pl.ds(pl.multiple_of(index * HALF, HALF), HALF)

    loads = [
        (tok_h, tok), (gmix_h, gmix),
        (wq_h, wq.at[:, 0:128]), (wk_h, wq.at[:, 128:256]), (wv_h, wq.at[:, 256:384]), (wo_h, wq.at[:, 384:512]),
        (wi_h, wi), (wf_h, wf), (fb_h, fb), (smax_h, smax), (sn_h, sn), (st_h, st), (wp_h, wp), (gffn_h, gffn),
        (wbr_h, wbr), (rt_h, rt), (rw_h, rw), (dg_h, dgu.at[:, 0:512]), (du_h, dgu.at[:, 512:1024]), (dd_h, dd),
        (eg_h.at[0], eg), (eu_h.at[0], eu), (ed_h.at[0], ed),
    ]
    copies = [pltpu.make_async_copy(s, d, load_sem.at[i]) for i, (s, d) in enumerate(loads)]
    for copy in copies:
        copy.start()

    barrier = pltpu.get_barrier_semaphore()

    def greet_ep(p):
        pl.semaphore_signal(barrier, inc=1, device_id=(p, t), device_id_type=MESH)

    def greet_tp(d, carry):
        pl.semaphore_signal(barrier, inc=1, device_id=(e, lax.rem(t + d, N)), device_id_type=MESH)
        return carry

    over_ep(greet_ep)
    lax.fori_loop(1, N, greet_tp, 0)
    copies[0].wait()
    copies[1].wait()
    pl.semaphore_wait(barrier, 2 * (N - 1))

    over_ep(lambda p: rcopy(tok.at[:, cols(p)], xall.at[e], ssem.at[0], bsem.at[e], p, t).start())
    xall[e] = tok[:, cols(e)]
    gain_e = gmix[:, cols(e)]

    total = jnp.zeros((ROWS, 128), F32)
    for k in range(8):
        wide = tok[:, k * 512:(k + 1) * 512].astype(F32)
        sq = wide * wide
        total = total + (sq[:, 0:128] + sq[:, 128:256]) + (sq[:, 256:384] + sq[:, 384:512])
    rstd = lax.rsqrt(jnp.sum(total, axis=1, keepdims=True) * (1.0 / D) + EPS)
    for i in (6, 7, 8, 9, 15, 16):
        copies[i].wait()
    gi = jnp.zeros((ROWS, N), F32)
    gf = jnp.zeros((ROWS, N), F32)
    for k in range(8):
        cut = slice(k * 512, (k + 1) * 512)
        nb = (tok[:, cut].astype(F32) * rstd * gmix[:, cut]).astype(BF16)
        gi = gi + dot(nb, wi[cut, :])
        gf = gf + dot(nb, wf[cut, :])
    gf = gf + fb[...]
    mine = lax.broadcasted_iota(jnp.int32, (ROWS, N), 1) == t
    gate_in = jnp.sum(jnp.where(mine, gi, 0.0), axis=1, keepdims=True)
    gate_f = jnp.sum(jnp.where(mine, gf, 0.0), axis=1, keepdims=True)
    log_keep = jnp.minimum(gate_f, 0.0) - jnp.log1p(jnp.exp(-jnp.abs(gate_f)))
    kept = log_keep + smax[...]
    new_max = jnp.maximum(kept, gate_in)
    keep = jnp.exp(kept - new_max)
    write = jnp.exp(gate_in - new_max)
    nmaxv[...] = new_max
    lane = lax.broadcasted_iota(jnp.int32, (ROWS, 128), 1)
    r_in = rt[...].astype(F32)
    w_in = rw[...]
    packed = jnp.where(lane == 0, r_in[:, 0:1], jnp.where(lane == 1, r_in[:, 1:2], jnp.where(lane == 2, w_in[:, 0:1], w_in[:, 1:2])))
    wide_rt = jnp.concatenate([packed, jnp.full((96, 128), -1.0, F32)], axis=0)
    rtsend[...] = jnp.transpose(wide_rt)[0:8, :]
    over_ep(lambda p: rcopy(rtsend, rtall.at[e], ssem.at[1], rsem.at[0], p, t).start())
    rtall[e] = rtsend[...]
    for i in (2, 3, 4, 5, 10, 11):
        copies[i].wait()

    for g in range(4):
        ps = [down(4 * g + j) for j in range(4)]
        for j in range(4):
            if 4 * g + j:
                wait_for(xall.at[ps[j]], bsem.at[ps[j]])
        block = jnp.concatenate([xall[p] for p in ps], axis=0)
        prod = dot((block.astype(F32) * gain_e).astype(BF16), wq[...])
        for j in range(4):
            piece = prod[32 * j:32 * j + 32].astype(BF16)
            if 4 * g + j:
                csend[ps[j]] = piece
                rcopy(csend.at[ps[j]], crecv.at[e], ssem.at[2], rsem.at[1], ps[j], t).start()
            else:
                crecv[e] = piece
    wait_for(crecv.at[0:15], rsem.at[1])
    qkvo = crecv[0].astype(F32)
    for i in range(1, N):
        qkvo = qkvo + crecv[i].astype(F32)
    qkvo = qkvo * rstd
    q = qkvo[:, 0:128]
    kw = qkvo[:, 128:256] * (HD ** -0.5) * write
    v = qkvo[:, 256:384]
    keep_w = jnp.broadcast_to(keep, (ROWS, HD))
    new_norm = keep_w * sn[...] + kw
    nnv[...] = new_norm
    kw_t = jnp.transpose(kw)
    q_t = jnp.transpose(q)
    for b in range(ROWS):
        new = keep_w[b:b + 1, :] * st[b] + kw_t[:, b:b + 1] * v[b:b + 1, :]
        st[b] = new
        num[b:b + 1, :] = jnp.sum(q_t[:, b:b + 1] * new, axis=0, keepdims=True)
    denom = jnp.maximum(jnp.abs(jnp.sum(q * new_norm, axis=1, keepdims=True)), 1.0)
    mixed = (jax.nn.sigmoid(qkvo[:, 384:512]) * (num[...] / denom)).astype(BF16)
    mhall[e] = mixed
    over_ep(lambda p: rcopy(mhall.at[e], mhall.at[e], ssem.at[3], rsem.at[2], p, t).start())
    stores = [
        pltpu.make_async_copy(st, nm_h, store_sem.at[0]),
        pltpu.make_async_copy(nnv, nn_h, store_sem.at[1]),
        pltpu.make_async_copy(nmaxv, nmax_h, store_sem.at[2]),
    ]
    for store in stores:
        store.start()

    wait_for(rtall.at[0:15], rsem.at[0])
    before = (lax.broadcasted_iota(jnp.int32, (128, 128), 0) < lax.broadcasted_iota(jnp.int32, (128, 128), 1)).astype(BF16)
    row8 = lax.broadcasted_iota(jnp.int32, (128, 128), 0)
    row_e = (row8 // 8).astype(F32)
    row_s = lax.rem(row8, 8).astype(F32)

    def table(group):
        info = rtall[group]
        first = (info[0:1, :] == row_e).astype(F32)
        second = (info[1:2, :] == row_e).astype(F32)
        slot = dot((first + second).astype(BF16), before)
        fits = (slot == row_s).astype(F32)
        share = 1.0 / (info[2:3, :] + info[3:4, :])
        pick = (first + second) * fits
        weigh = (first * (info[2:3, :] * share) + second * (info[3:4, :] * share)) * fits
        return pick[:, 0:ROWS], weigh

    pick0, weigh0 = table(2 * z)
    pick1, weigh1 = table(2 * z + 1)
    weigh = jnp.where(c == 0, weigh0, weigh1)
    weigh_t = jnp.transpose(weigh)[0:ROWS, :]

    copies[12].wait()
    wait_for(mhall.at[0:15], rsem.at[2])

    def reduce_tp(parts, recv, send, zrecv, s, r):
        copy = rcopy(parts.at[:, 1 - c], recv, ssem.at[s], rsem.at[r], e, mate)
        copy.start()
        wait_for(recv, rsem.at[r])
        for k in range(NZ):
            send[k] = (parts[k, c].astype(F32) + recv[k].astype(F32)).astype(BF16)
        over_z(lambda p: rcopy(send.at[p], zrecv.at[z], ssem.at[s + 1], rsem.at[r + 1], e, 2 * p + c).start())
        zrecv[z] = send[z]

    def total_tp(zrecv, r):
        wait_for(zrecv.at[0:7], rsem.at[r + 1])
        tot = zrecv[0].astype(F32)
        for k in range(1, NZ):
            tot = tot + zrecv[k].astype(F32)
        return tot

    for g in range(4):
        block = jnp.concatenate([mhall[4 * g + j] for j in range(4)], axis=0)
        prod = dot(block, wp[...])
        for j in range(4):
            b = 4 * g + j
            part[b // 2, b % 2] = prod[32 * j:32 * j + 32].astype(BF16)
    reduce_tp(part, pd2d, rsend, rrecv, 4, 3)
    mix = total_tp(rrecv, 3)
    res_own = (xall[t].astype(F32) + mix).astype(BF16)
    resall[z, c] = res_own

    rcopy(resall.at[z, c], resall.at[z, c], ssem.at[6], z2sem.at[0, z], e, mate).start()
    over_z(lambda p: rcopy(resall.at[z, c], resall.at[z, c], ssem.at[7], zsem.at[0, z], e, 2 * p + c).start())
    wait_for(resall.at[z, 1 - c], z2sem.at[0, z])
    both = jnp.concatenate([resall[z, 0], resall[z, 1]], axis=0)
    zero = jnp.zeros((8, ROWS), F32)
    spread = []
    for ex in range(N):
        spread.append(jnp.concatenate([pick0[8 * ex:8 * ex + 8], zero], axis=1))
        spread.append(jnp.concatenate([zero, pick1[8 * ex:8 * ex + 8]], axis=1))
    routed = dot(jnp.concatenate(spread, axis=0).astype(BF16), both).astype(BF16)
    for ex in range(N):
        xs[ex] = routed[16 * ex:16 * ex + 16]
    over_ep(lambda p: rcopy(xs.at[p], xfull.at[z, :, cols(e)], ssem.at[8], rsem.at[5], p, t).start())
    xfull[z, :, cols(e)] = xs[e]

    for i in (13, 14, 17, 18):
        copies[i].wait()
    for d in range(1, NZ):
        p = lax.rem(z + NZ - d, NZ)
        wait_for(resall.at[p, c], zsem.at[0, p])
        rcopy(resall.at[p, c], resall.at[p, c], ssem.at[9], z2sem.at[0, p], e, mate).start()

    wait_for(xs.at[0:15], rsem.at[5])
    over_z(lambda p: rcopy(xfull.at[z, :, half(c)], xfull.at[z, :, half(c)], ssem.at[10], zsem.at[1, z], e, 2 * p + c).start())

    gain_f = gffn[:, cols(e)]
    w_b = wbr[:, cols(e)].astype(BF16)
    for d in range(1, NZ):
        p = lax.rem(z + NZ - d, NZ)
        wait_for(resall.at[p, 1 - c], z2sem.at[0, p])
    for k in range(NZ):
        wide = jnp.concatenate([resall[k, 0], resall[k, 1]], axis=0).astype(F32)
        r2all[64 * k:64 * k + 64] = (wide * wide).astype(BF16)
        aall[64 * k:64 * k + 64] = (wide * gain_f).astype(BF16)

    def dense_block(g, carry):
        rows = pl.ds(pl.multiple_of(g * 128, 128), 128)
        lhs = aall[rows, :]
        for h in range(2):
            prod = dot(lhs, dgu[:, 512 * h:512 * h + 512])
            for j in range(4):
                dsend[4 * g + j, :, 512 * h:512 * h + 512] = prod[32 * j:32 * j + 32].astype(BF16)
        stat = dot_rows(jnp.ones((8, COLS), BF16), r2all[rows, :])
        br = dot_rows(jnp.broadcast_to(w_b, (8, COLS)), lhs)
        sub = lax.broadcasted_iota(jnp.int32, (8, 128), 0)
        stsend[g] = jnp.where(sub < 4, stat, br)
        return carry

    lax.fori_loop(0, 4, dense_block, 0)
    over_ep(lambda p: rcopy(dsend.at[p], drecv.at[e], ssem.at[11], rsem.at[6], p, t).start())
    over_ep(lambda p: rcopy(stsend.at[p // 4], strecv.at[e], ssem.at[12], rsem.at[7], p, t).start())
    drecv[e] = dsend[e]
    strecv[e] = stsend[e // 4]

    for d in range(1, NZ):
        p = lax.rem(z + NZ - d, NZ)
        wait_for(xfull.at[p, :, half(c)], zsem.at[1, p])
        rcopy(xfull.at[p, :, half(c)], xfull.at[p, :, half(c)], ssem.at[13], z2sem.at[1, p], e, mate).start()

    wait_for(drecv.at[0:15], rsem.at[6])
    wait_for(strecv.at[0:15], rsem.at[7])
    stats = strecv[0]
    for i in range(1, N):
        stats = stats + strecv[i]
    at = lane == lax.broadcasted_iota(jnp.int32, (ROWS, 128), 0) + ROWS * lax.rem(e, 4)
    sumsq = jnp.sum(jnp.where(at, stats[0:1, :], 0.0), axis=1, keepdims=True)
    branch = jnp.sum(jnp.where(at, stats[4:5, :], 0.0), axis=1, keepdims=True)
    rstd2 = lax.rsqrt(sumsq * (1.0 / D) + EPS)
    branch_share = jax.nn.sigmoid(branch * rstd2)
    for h in range(2):
        cg = slice(256 * h, 256 * h + 256)
        cu = slice(512 + 256 * h, 512 + 256 * h + 256)
        g_ = drecv[0, :, cg].astype(F32)
        u_ = drecv[0, :, cu].astype(F32)
        for i in range(1, N):
            g_ = g_ + drecv[i, :, cg].astype(F32)
            u_ = u_ + drecv[i, :, cu].astype(F32)
        g_ = g_ * rstd2
        u_ = u_ * rstd2
        hall[e, :, cg] = (g_ * jax.nn.sigmoid(g_) * u_ * branch_share).astype(BF16)
    over_ep(lambda p: rcopy(hall.at[e], hall.at[e], ssem.at[14], rsem.at[8], p, t).start())

    for i in (20, 21, 22):
        copies[i].wait()
    for d in range(1, NZ):
        p = lax.rem(z + NZ - d, NZ)
        wait_for(xfull.at[p, :, half(1 - c)], z2sem.at[1, p])

    def expert_rows(k, carry):
        tot = jnp.zeros((16, 128), F32)
        for m in range(4):
            wide = xfull[k, :, 1024 * m:1024 * m + 1024].astype(F32)
            sq = wide * wide
            for n in range(8):
                tot = tot + sq[:, 128 * n:128 * n + 128]
        scale = lax.rsqrt(jnp.sum(tot, axis=1, keepdims=True) * (1.0 / D) + EPS)
        rows = pl.ds(pl.multiple_of(k * 16, 16), 16)
        for m in range(4):
            cut = slice(1024 * m, 1024 * m + 1024)
            aexp[rows, cut] = (xfull[k, :, cut].astype(F32) * scale * gffn[:, cut]).astype(BF16)
        return carry

    lax.fori_loop(0, NZ, expert_rows, 0)
    acc[...] = jnp.zeros_like(acc)

    def expert_in(k, carry):
        cut = pl.ds(pl.multiple_of(k * 512, 512), 512)
        lhs = aexp[:, cut]
        acc[:, 0:256] += dot(lhs, eg[cut, :])
        acc[:, 256:512] += dot(lhs, eu[cut, :])
        return carry

    lax.fori_loop(0, 8, expert_in, 0)
    g_ = acc[:, 0:256]
    hid = (g_ * jax.nn.sigmoid(g_) * acc[:, 256:512]).astype(BF16)
    aexp[:, 0:256] = hid

    def expert_out(k, carry):
        cut = pl.ds(pl.multiple_of(k * 512, 512), 512)
        prod = dot(aexp[:, 0:256], ed[:, cut]).astype(BF16)
        for n in range(NZ):
            yp[n, :, cut] = prod[16 * n:16 * n + 16]
        return carry

    lax.fori_loop(0, 8, expert_out, 0)
    rcopy(yp.at[:, :, half(1 - c)], yd2d, ssem.at[15], rsem.at[9], e, mate).start()

    copies[19].wait()
    wait_for(hall.at[0:15], rsem.at[8])

    def dense_down(g, carry):
        block = jnp.concatenate([hall[4 * g + j] for j in range(4)], axis=0)
        prod = dot(block, dd[...])
        for j in range(4):
            part2[2 * g + j // 2, j % 2] = prod[32 * j:32 * j + 32].astype(BF16)
        return carry

    lax.fori_loop(0, 4, dense_down, 0)
    reduce_tp(part2, pd2d2, rsend2, rrecv2, 16, 10)

    wait_for(yd2d, rsem.at[9])

    def sum_pair(k, carry):
        ys[k] = (yp[k, :, half(c)].astype(F32) + yd2d[k].astype(F32)).astype(BF16)
        return carry

    lax.fori_loop(0, NZ, sum_pair, 0)
    over_z(lambda p: rcopy(ys.at[p], yrecv.at[z], ssem.at[18], rsem.at[12], e, 2 * p + c).start())
    yrecv[z] = ys[z]
    dense = total_tp(rrecv2, 10)
    wait_for(yrecv.at[0:7], rsem.at[12])
    for m in range(4):
        cut = slice(512 * m, 512 * m + 512)
        tot = yrecv[0, :, cut].astype(F32)
        for k in range(1, NZ):
            tot = tot + yrecv[k, :, cut].astype(F32)
        yout[:, cut] = tot.astype(BF16)

    def back(j, carry):
        src = yout.at[:, pl.ds(pl.multiple_of(j * COLS, COLS), COLS)]
        pe = c * NZ + j
        rcopy(src, ycomb.at[e], ssem.at[19], rsem.at[13], pe, mate).start()

        @pl.when(pe != e)
        def _():
            rcopy(src, ycomb.at[e], ssem.at[20], rsem.at[13], pe, t).start()

        @pl.when(pe == e)
        def _():
            ycomb[e] = yout[:, pl.ds(pl.multiple_of(j * COLS, COLS), COLS)]

        return carry

    lax.fori_loop(0, NZ, back, 0)
    either(e // NZ == c, ycomb.at[0:15], ycomb, rsem.at[13])

    picked = jnp.concatenate([ycomb[ex, :, :] for ex in range(N)], axis=0).astype(F32)
    own = jnp.concatenate([picked[16 * ex:16 * ex + 16].reshape(2, 8, COLS) for ex in range(N)], axis=0)
    sel = jnp.concatenate(
        [jnp.where(c == 0, own[2 * ex], own[2 * ex + 1]) for ex in range(N)], axis=0
    )
    high = weigh_t.astype(BF16)
    low = (weigh_t - high.astype(F32)).astype(BF16)
    sel16 = sel.astype(BF16)
    mixed_out = dot(high, sel16) + dot(low, sel16)
    outv[...] = (resall[z, c].astype(F32) + mixed_out + dense).astype(BF16)

    def deliver(d, carry):
        pt = lax.rem(t + d, N)

        @pl.when(jnp.logical_or(t != e, pt != t))
        def _():
            rcopy(outv, out_h.at[:, cols(e)], ssem.at[21], rsem.at[14], t, pt).start()

        return carry

    lax.fori_loop(0, N, deliver, 0)

    @pl.when(t == e)
    def _():
        own_copy = pltpu.make_async_copy(outv, out_h.at[:, cols(e)], store_sem.at[3])
        own_copy.start()
        own_copy.wait()

    either(t == e, out_h.at[:, 0:15 * COLS], out_h, rsem.at[14])

    wait_for(xall.at[0:15], ssem.at[0])
    wait_for(rtall.at[0:15], ssem.at[1])
    wait_for(csend.at[0:15], ssem.at[2])
    wait_for(mhall.at[0:15], ssem.at[3])
    wait_for(pd2d, ssem.at[4])
    wait_for(rsend.at[0:7], ssem.at[5])
    wait_for(resall.at[0, 0], ssem.at[6])
    wait_for(rsend.at[0:7], ssem.at[7])
    wait_for(xs.at[0:15], ssem.at[8])
    wait_for(rsend.at[0:7], ssem.at[9])
    wait_for(ys.at[0:7], ssem.at[10])
    wait_for(dsend.at[0:15], ssem.at[11])
    wait_for(strecv.at[0:15], ssem.at[12])
    wait_for(ys.at[0:7], ssem.at[13])
    wait_for(hall.at[0:15], ssem.at[14])
    wait_for(yd2d, ssem.at[15])
    wait_for(pd2d2, ssem.at[16])
    wait_for(rsend2.at[0:7], ssem.at[17])
    wait_for(ys.at[0:7], ssem.at[18])
    wait_for(ycomb.at[0:8], ssem.at[19])
    either(e // NZ == c, ycomb.at[0:7], ycomb.at[0:8], ssem.at[20])

    either(t == e, xall.at[0:15], xall, ssem.at[21])

    for store in stores:
        store.wait()


def on_device(
    tokens, state_matrix, state_norm, state_max, mixer_gain, w_query, w_key, w_value, w_outgate, w_ingate, w_forget,
    forget_bias, w_proj, ffn_gain, w_branch, routes, route_weight, expert_gate, expert_up, expert_down,
    dense_gate, dense_up, dense_down,
):
    any_ = pl.BlockSpec(memory_space=pl.ANY)
    vm = pltpu.VMEM
    scratch = [
        vm((ROWS, D), BF16), vm((ROWS, HD, HD), F32), vm((ROWS, HD), F32), vm((ROWS, 1), F32), vm((1, D), F32),
        vm((COLS, 512), BF16), vm((D, N), BF16), vm((D, N), BF16), vm((1, N), F32), vm((HD, COLS), BF16),
        vm((1, D), F32), vm((1, D), F32), vm((ROWS, 2), jnp.int32), vm((ROWS, 2), F32),
        vm((D, COLS), BF16), vm((D, COLS), BF16), vm((COLS, D), BF16), vm((COLS, 1024), BF16), vm((512, COLS), BF16),
        vm((N, ROWS, COLS), BF16), vm((N, ROWS, 512), BF16), vm((N, ROWS, 512), BF16), vm((N, ROWS, HD), BF16),
        vm((ROWS, HD), F32),
        vm((NZ, 2, ROWS, COLS), BF16), vm((NZ, ROWS, COLS), BF16), vm((NZ, ROWS, COLS), BF16),
        vm((NZ, ROWS, COLS), BF16), vm((NZ, 2, ROWS, COLS), BF16),
        vm((NZ, 2, ROWS, COLS), BF16), vm((NZ, ROWS, COLS), BF16), vm((NZ, ROWS, COLS), BF16),
        vm((NZ, ROWS, COLS), BF16),
        vm((8, 128), F32), vm((N, 8, 128), F32), vm((N, ROWS, 1024), BF16), vm((N, ROWS, 1024), BF16),
        vm((4, 8, 128), F32), vm((N, 8, 128), F32), vm((N, ROWS, 512), BF16), vm((512, COLS), BF16),
        vm((512, COLS), BF16),
        vm((N, 16, COLS), BF16), vm((NZ, 16, D), BF16), vm((128, D), BF16), vm((128, 512), F32),
        vm((NZ, 16, D), BF16), vm((NZ, 16, HALF), BF16), vm((NZ, 16, HALF), BF16), vm((NZ, 16, HALF), BF16),
        vm((16, HALF), BF16), vm((N, 16, COLS), BF16), vm((ROWS, COLS), BF16), vm((ROWS, HD), F32), vm((ROWS, 1), F32),
        pltpu.SemaphoreType.DMA((23,)), pltpu.SemaphoreType.DMA((22,)), pltpu.SemaphoreType.DMA((N,)),
        pltpu.SemaphoreType.DMA((15,)), pltpu.SemaphoreType.DMA((2, NZ)), pltpu.SemaphoreType.DMA((2, NZ)),
        pltpu.SemaphoreType.DMA((4,)),
    ]
    out, nm, nn, nmax = pl.pallas_call(
        layer_kernel,
        out_shape=(
            jax.ShapeDtypeStruct((ROWS, D), BF16),
            jax.ShapeDtypeStruct((ROWS, HD, HD), F32),
            jax.ShapeDtypeStruct((ROWS, HD), F32),
            jax.ShapeDtypeStruct((ROWS, 1), F32),
        ),
        in_specs=[any_] * 23,
        out_specs=(any_,) * 4,
        scratch_shapes=scratch,
        compiler_params=pltpu.CompilerParams(
            collective_id=0, has_side_effects=True, vmem_limit_bytes=60 * 1024 * 1024
        ),
        name="layer",
    )(
        tokens, state_matrix.reshape(ROWS, HD, HD), state_norm.reshape(ROWS, HD), state_max,
        mixer_gain.reshape(1, D), w_query, w_key, w_value, w_outgate, w_ingate, w_forget,
        forget_bias.reshape(1, N), w_proj, ffn_gain.reshape(1, D), w_branch.astype(F32).reshape(1, D), routes,
        route_weight, expert_gate, expert_up, expert_down, dense_gate, dense_up, dense_down,
    )
    return (
        out, nm.reshape(ROWS, 1, HD, HD), nn.reshape(ROWS, 1, HD), nmax,
    )


def solution(mesh):
    in_specs = (
        P("ep", None), P("ep", "tp", None, None), P("ep", "tp", None), P("ep", "tp"), P(),
        P("ep", "tp"), P("ep", "tp"), P("ep", "tp"), P("ep", "tp"), P(), P(), P(), P("tp", "ep"), P(), P(),
        P("ep", None), P("ep", None), P("ep", None, "tp"), P("ep", None, "tp"), P("ep", "tp", None),
        P("ep", "tp"), P("ep", "tp"), P("tp", "ep"),
    )
    out_specs = (P("ep", None), P("ep", "tp", None, None), P("ep", "tp", None), P("ep", "tp"))
    return jax.shard_map(on_device, mesh=mesh, in_specs=in_specs, out_specs=out_specs, check_vma=False)
```

```python
import functools

import jax
import jax.numpy as jnp
from jax import lax
from jax.experimental import pallas as pl
from jax.experimental.pallas import tpu as pltpu
from jax.sharding import PartitionSpec as P

EPS = 1e-06
MESH = pl.DeviceIdType.MESH
F32 = jnp.float32
BF16 = jnp.bfloat16
N = 16
NZ = 8
ROWS = 32
D = 4096
COLS = 256
HALF = 2048
HD = 128
SECOND_AT = 4


def dot(a, b):
    return jnp.dot(a, b, preferred_element_type=F32)


def dot_rows(a, b):
    return lax.dot_general(a, b, (((1,), (1,)), ((), ())), preferred_element_type=F32)


def layer_kernel(
    tok_h, st_h, sn_h, smax_h, gmix_h, wq_h, wk_h, wv_h, wo_h, wi_h, wf_h, fb_h, wp_h, gffn_h, wbr_h,
    rt_h, rw_h, eg_h, eu_h, ed_h, dg_h, du_h, dd_h,
    out_h, nm_h, nn_h, nmax_h,
    tok, st, sn, smax, gmix, wq, wi, wf, fb, wp, gffn, wbr, rt, rw, eg, eu, ed, dgu, dd,
    xall, csend, crecv, mhall, heads, num,
    wpall, wtab, resall,
    part2, pd2d2, rsend2, rrecv2,
    rtsend, rtall, dsg, dsu, r1g, r1u, d2g, d2u, r2g, r2u, stsend, strecv, hall, r2all, aall,
    xs, xfull, aexp, acc, yp, yd2d, ys, yin, outv, ofull, nnv, nmaxv,
    load_sem, ssem, bsem, rsem, zsem, z2sem, osem, hsem, gsem, store_sem,
):
    e = lax.axis_index("ep")
    t = lax.axis_index("tp")
    z = t // 2
    c = lax.rem(t, 2)
    mate = 2 * z + 1 - c

    def rcopy(src, dst, send, recv, pe, pt):
        return pltpu.make_async_remote_copy(
            src_ref=src, dst_ref=dst, send_sem=send, recv_sem=recv, device_id=(pe, pt), device_id_type=MESH
        )

    def wait_for(ref, sem):
        pltpu.make_async_copy(ref, ref, sem).wait()

    def either(less, ref_less, ref_all, sem):
        @pl.when(less)
        def _():
            wait_for(ref_less, sem)

        @pl.when(jnp.logical_not(less))
        def _():
            wait_for(ref_all, sem)

    def up(d):
        return lax.rem(e + d, N)

    def down(d):
        return lax.rem(e + N - d, N)

    def over_ep(fn):
        lax.fori_loop(1, N, lambda d, carry: (fn(up(d)), carry)[1], 0)

    def over_z(fn):
        lax.fori_loop(1, NZ, lambda d, carry: (fn(lax.rem(z + d, NZ)), carry)[1], 0)

    def cols(index):
        return pl.ds(pl.multiple_of(index * COLS, COLS), COLS)

    def half(index):
        return pl.ds(pl.multiple_of(index * HALF, HALF), HALF)

    scopes = []

    def mark(name):
        if scopes:
            scopes.pop().__exit__(None, None, None)
        if name:
            scopes.append(jax.named_scope(name))
            scopes[-1].__enter__()

    mark("a_barrier")
    loads = [
        (tok_h, tok), (gmix_h, gmix),
        (wq_h, wq.at[:, 0:128]), (wk_h, wq.at[:, 128:256]), (wv_h, wq.at[:, 256:384]), (wo_h, wq.at[:, 384:512]),
        (wi_h, wi), (wf_h, wf), (fb_h, fb), (smax_h, smax), (sn_h, sn), (st_h, st), (wp_h, wp), (gffn_h, gffn),
        (wbr_h, wbr), (rt_h, rt), (rw_h, rw), (dg_h, dgu.at[:, 0:512]), (du_h, dgu.at[:, 512:1024]), (dd_h, dd),
        (eg_h.at[0], eg), (eu_h.at[0], eu), (ed_h.at[0], ed),
    ]
    copies = [pltpu.make_async_copy(s, d, load_sem.at[i]) for i, (s, d) in enumerate(loads)]
    for copy in copies:
        copy.start()

    barrier = pltpu.get_barrier_semaphore()

    def greet_ep(p):
        pl.semaphore_signal(barrier, inc=1, device_id=(p, t), device_id_type=MESH)

    def greet_tp(d, carry):
        pl.semaphore_signal(barrier, inc=1, device_id=(e, lax.rem(t + d, N)), device_id_type=MESH)
        return carry

    over_ep(greet_ep)
    lax.fori_loop(1, N, greet_tp, 0)
    copies[0].wait()
    copies[1].wait()
    pl.semaphore_wait(barrier, 2 * (N - 1))

    mark("b_spread_gates")
    over_ep(lambda p: rcopy(tok.at[:, cols(p)], xall.at[e], ssem.at[0], bsem.at[e], p, t).start())
    copies[12].wait()
    mine_wp = wpall.at[pl.ds(pl.multiple_of(t * HD, HD), HD), :]
    rcopy(wp, mine_wp, ssem.at[4], z2sem.at[2, z], e, mate).start()
    over_z(lambda p: rcopy(wp, mine_wp, ssem.at[5], zsem.at[2, z], e, 2 * p + c).start())
    wpall[pl.ds(pl.multiple_of(t * HD, HD), HD), :] = wp[...]
    xall[e] = tok[:, cols(e)]
    gain_e = gmix[:, cols(e)]

    total = jnp.zeros((ROWS, 128), F32)
    for k in range(8):
        wide = tok[:, k * 512:(k + 1) * 512].astype(F32)
        sq = wide * wide
        total = total + (sq[:, 0:128] + sq[:, 128:256]) + (sq[:, 256:384] + sq[:, 384:512])
    rstd = lax.rsqrt(jnp.sum(total, axis=1, keepdims=True) * (1.0 / D) + EPS)
    for i in (6, 7, 8, 9, 15, 16):
        copies[i].wait()
    gi = jnp.zeros((ROWS, N), F32)
    gf = jnp.zeros((ROWS, N), F32)
    for k in range(8):
        cut = slice(k * 512, (k + 1) * 512)
        nb = (tok[:, cut].astype(F32) * rstd * gmix[:, cut]).astype(BF16)
        gi = gi + dot_rows(nb, wi[:, cut])
        gf = gf + dot_rows(nb, wf[:, cut])
    gf = gf + fb[...]
    mine = lax.broadcasted_iota(jnp.int32, (ROWS, N), 1) == t
    gate_in = jnp.sum(jnp.where(mine, gi, 0.0), axis=1, keepdims=True)
    gate_f = jnp.sum(jnp.where(mine, gf, 0.0), axis=1, keepdims=True)
    log_keep = jnp.minimum(gate_f, 0.0) - jnp.log1p(jnp.exp(-jnp.abs(gate_f)))
    square = lax.broadcasted_iota(jnp.int32, (ROWS, ROWS), 0) == lax.broadcasted_iota(jnp.int32, (ROWS, ROWS), 1)
    kept = log_keep + jnp.sum(jnp.where(square, smax[...], 0.0), axis=1, keepdims=True)
    new_max = jnp.maximum(kept, gate_in)
    keep = jnp.exp(kept - new_max)
    write = jnp.exp(gate_in - new_max)
    nmaxv[...] = jnp.sum(jnp.where(square, new_max, 0.0), axis=0, keepdims=True)
    rtsend[...] = jnp.full((8, 128), -1.0, F32)
    rtsend[0:2, 0:ROWS] = rt[...].astype(F32)
    rtsend[2:4, 0:ROWS] = rw[...]
    over_ep(lambda p: rcopy(rtsend, rtall.at[e], ssem.at[1], rsem.at[0], p, t).start())
    rtall[e] = rtsend[...]
    for i in (2, 3, 4, 5, 10, 11):
        copies[i].wait()

    mark("c_qkvo_part")
    for g in range(4):
        ps = [down(4 * g + j) for j in range(4)]
        for j in range(4):
            if 4 * g + j:
                wait_for(xall.at[ps[j]], bsem.at[ps[j]])
        block = jnp.concatenate([xall[p] for p in ps], axis=0)
        prod = dot((block.astype(F32) * gain_e).astype(BF16), wq[...])
        for j in range(4):
            piece = prod[32 * j:32 * j + 32].astype(BF16)
            if 4 * g + j:
                csend[ps[j]] = piece
                rcopy(csend.at[ps[j]], crecv.at[e], ssem.at[2], rsem.at[1], ps[j], t).start()
            else:
                crecv[e] = piece
    mark("d_wait_qkvo")
    wait_for(crecv.at[0:15], rsem.at[1])
    mark("e_cell")
    qkvo = crecv[0].astype(F32)
    for i in range(1, N):
        qkvo = qkvo + crecv[i].astype(F32)
    qkvo = qkvo * rstd
    q = qkvo[:, 0:128]
    kw = qkvo[:, 128:256] * (HD ** -0.5) * write
    v = qkvo[:, 256:384]
    keep_w = jnp.broadcast_to(keep, (ROWS, HD))
    new_norm = keep_w * sn[...] + kw
    nnv[...] = new_norm
    kw_t = jnp.transpose(kw)
    q_t = jnp.transpose(q)
    for b in range(ROWS):
        new = keep_w[b:b + 1, :] * st[b] + kw_t[:, b:b + 1] * v[b:b + 1, :]
        st[b] = new
        num[b:b + 1, :] = jnp.sum(q_t[:, b:b + 1] * new, axis=0, keepdims=True)
    denom = jnp.maximum(jnp.abs(jnp.sum(q * new_norm, axis=1, keepdims=True)), 1.0)
    mhall[e] = (jax.nn.sigmoid(qkvo[:, 384:512]) * (num[...] / denom)).astype(BF16)
    over_ep(lambda p: rcopy(mhall.at[e], mhall.at[e], ssem.at[23], hsem.at[e], p, t).start())
    head_cols = pl.ds(pl.multiple_of(t * HD, HD), HD)

    def turn_heads(d, carry):
        p = down(d)

        @pl.when(d > 0)
        def _():
            wait_for(mhall.at[p], hsem.at[p])

        @pl.when(p != t)
        def _():
            rcopy(mhall.at[p], heads.at[:, head_cols], ssem.at[3], rsem.at[2], e, p).start()

        @pl.when(p == t)
        def _():
            heads[:, head_cols] = mhall[p]

        return carry

    stores = [
        pltpu.make_async_copy(st, nm_h, store_sem.at[0]),
        pltpu.make_async_copy(nnv, nn_h, store_sem.at[1]),
        pltpu.make_async_copy(nmaxv, nmax_h, store_sem.at[2]),
    ]
    for store in stores:
        store.start()

    mark("f_tables")
    wait_for(rtall.at[0:15], rsem.at[0])
    before = (lax.broadcasted_iota(jnp.int32, (128, 128), 0) < lax.broadcasted_iota(jnp.int32, (128, 128), 1)).astype(BF16)
    row8 = lax.broadcasted_iota(jnp.int32, (128, 128), 0)
    row_e = (row8 // 8).astype(F32)
    row_s = lax.rem(row8, 8).astype(F32)

    def table(group):
        info = rtall[group]
        first = (info[0:1, :] == row_e).astype(F32)
        second = (info[1:2, :] == row_e).astype(F32)
        slot = dot((first + second).astype(BF16), before)
        fits = (slot == row_s).astype(F32)
        share = 1.0 / (info[2:3, :] + info[3:4, :])
        pick = (first + second) * fits
        weigh = (first * (info[2:3, :] * share) + second * (info[3:4, :] * share)) * fits
        return pick[:, 0:ROWS], weigh

    pick0 = table(2 * z)[0]
    pick1 = table(2 * z + 1)[0]

    def wp_rows(index):
        return wpall.at[pl.ds(pl.multiple_of(index * HD, HD), HD), :]

    for d in range(1, NZ):
        p = lax.rem(z + NZ - d, NZ)
        wait_for(wp_rows(2 * p + c), zsem.at[2, p])
        rcopy(wp_rows(2 * p + c), wp_rows(2 * p + c), ssem.at[21], z2sem.at[2, p], e, mate).start()
    lax.fori_loop(0, N, turn_heads, 0)
    mark("g_wait_heads")
    def combine_table(k, carry):
        turned = jnp.transpose(table(2 * k + c)[1])[0:ROWS, :]
        high = turned.astype(BF16)
        wtab[k, 0] = high
        wtab[k, 1] = (turned - high.astype(F32)).astype(BF16)
        return carry

    lax.fori_loop(0, NZ, combine_table, 0)

    for d in range(NZ):
        p = lax.rem(z + NZ - d, NZ)
        wait_for(wp_rows(2 * p + 1 - c), z2sem.at[2, p])

    wait_for(heads.at[:, 0:15 * HD], rsem.at[2])
    mark("h_proj")
    mix = dot(heads[...], wpall[...])
    res_own = (xall[t].astype(F32) + mix).astype(BF16)
    resall[z, c] = res_own

    mark("j_ag_send")
    rcopy(resall.at[z, c], resall.at[z, c], ssem.at[6], z2sem.at[0, z], e, mate).start()
    over_z(lambda p: rcopy(resall.at[z, c], resall.at[z, c], ssem.at[7], zsem.at[0, z], e, 2 * p + c).start())
    mark("k_wait_mate_dispatch")
    wait_for(resall.at[z, 1 - c], z2sem.at[0, z])
    both = jnp.concatenate([resall[z, 0], resall[z, 1]], axis=0)
    zero = jnp.zeros((8, ROWS), F32)
    spread = []
    for ex in range(N):
        spread.append(jnp.concatenate([pick0[8 * ex:8 * ex + 8], zero], axis=1))
        spread.append(jnp.concatenate([zero, pick1[8 * ex:8 * ex + 8]], axis=1))
    routed = dot(jnp.concatenate(spread, axis=0).astype(BF16), both).astype(BF16)
    for ex in range(N):
        xs[ex] = routed[16 * ex:16 * ex + 16]
    over_ep(lambda p: rcopy(xs.at[p], xfull.at[z, :, cols(e)], ssem.at[8], rsem.at[5], p, t).start())
    xfull[z, :, cols(e)] = xs[e]

    for i in (13, 14, 17, 18):
        copies[i].wait()
    mark("l_ag_forward")
    for d in range(1, NZ):
        p = lax.rem(z + NZ - d, NZ)
        wait_for(resall.at[p, c], zsem.at[0, p])
        rcopy(resall.at[p, c], resall.at[p, c], ssem.at[9], z2sem.at[0, p], e, mate).start()

    mark("m_wait_dispatch")
    wait_for(xs.at[0:15], rsem.at[5])
    over_z(lambda p: rcopy(xfull.at[z, :, half(c)], xfull.at[z, :, half(c)], ssem.at[10], zsem.at[1, z], e, 2 * p + c).start())

    mark("n_wait_fwd_dense")
    gain_f = gffn[:, cols(e)]
    sub = lax.broadcasted_iota(jnp.int32, (ROWS, HD), 0)
    w_rows = wbr[...].astype(F32)
    w_b = jnp.concatenate(
        [jnp.sum(jnp.where(sub == 2 * e + k, w_rows, 0.0), axis=0, keepdims=True) for k in range(2)], axis=1
    ).astype(BF16)
    for d in range(1, NZ):
        p = lax.rem(z + NZ - d, NZ)
        wait_for(resall.at[p, 1 - c], z2sem.at[0, p])
    for k in range(NZ):
        wide = jnp.concatenate([resall[k, 0], resall[k, 1]], axis=0).astype(F32)
        r2all[64 * k:64 * k + 64] = (wide * wide).astype(BF16)
        aall[64 * k:64 * k + 64] = (wide * gain_f).astype(BF16)

    def dense_block(g, carry):
        rows = pl.ds(pl.multiple_of(g * 128, 128), 128)
        lhs = aall[rows, :]
        for h in range(2):
            prod = dot(lhs, dgu[:, 512 * h:512 * h + 512])
            for j in range(4):
                piece = prod[32 * j:32 * j + 32].astype(BF16)
                if h == 0:
                    dsg[j, g] = piece
                else:
                    dsu[g, j] = piece
        stat = dot_rows(jnp.ones((8, COLS), BF16), r2all[rows, :])
        br = dot_rows(jnp.broadcast_to(w_b, (8, COLS)), lhs)
        sub = lax.broadcasted_iota(jnp.int32, (8, 128), 0)
        stsend[g] = jnp.where(sub < 4, stat, br)
        return carry

    lax.fori_loop(0, 4, dense_block, 0)
    ey, ex_ = e // 4, lax.rem(e, 4)
    for d in (2, 1, 3):
        px, py = lax.rem(ex_ + d, 4), lax.rem(ey + d, 4)
        rcopy(dsg.at[px], r1g.at[ex_], ssem.at[11], gsem.at[0], 4 * ey + px, t).start()
        rcopy(dsu.at[py], r1u.at[ey], ssem.at[24], gsem.at[1], 4 * py + ex_, t).start()
    over_ep(lambda p: rcopy(stsend.at[p // 4], strecv.at[e], ssem.at[12], rsem.at[7], p, t).start())
    r1g[ex_] = dsg[ex_]
    r1u[ey] = dsu[ey]
    strecv[e] = stsend[e // 4]

    mark("o_expert_fwd")
    def second_stage():
        for parts, got, mine, left, sem in ((r1g, d2g, ey, r2g, 0), (r1u, d2u, ex_, r2u, 1)):
            wait_for(parts.at[0:3], gsem.at[sem])
            for k in range(4):
                tot = parts[0, k].astype(F32) + parts[1, k].astype(F32)
                got[k] = (tot + parts[2, k].astype(F32) + parts[3, k].astype(F32)).astype(BF16)
            left[mine] = got[mine]
            for d in (2, 1, 3):
                other = lax.rem(mine + d, 4)
                target = 4 * other + ex_ if sem == 0 else 4 * ey + other
                rcopy(got.at[other], left.at[mine], ssem.at[25 + sem], gsem.at[2 + sem], target, t).start()

    for d in range(1, NZ):
        p = lax.rem(z + NZ - d, NZ)
        wait_for(xfull.at[p, :, half(c)], zsem.at[1, p])
        rcopy(xfull.at[p, :, half(c)], xfull.at[p, :, half(c)], ssem.at[13], z2sem.at[1, p], e, mate).start()
        if d == SECOND_AT:
            second_stage()

    mark("p_wait_dense")
    wait_for(r2g.at[0:3], gsem.at[2])
    wait_for(r2u.at[0:3], gsem.at[3])
    wait_for(strecv.at[0:15], rsem.at[7])
    mark("q_hidden")
    stats = strecv[0]
    for i in range(1, N):
        stats = stats + strecv[i]
    lane = lax.broadcasted_iota(jnp.int32, (ROWS, 128), 1)
    at = lane == lax.broadcasted_iota(jnp.int32, (ROWS, 128), 0) + ROWS * lax.rem(e, 4)
    sumsq = jnp.sum(jnp.where(at, stats[0:1, :], 0.0), axis=1, keepdims=True)
    branch = jnp.sum(jnp.where(at, stats[4:5, :], 0.0), axis=1, keepdims=True)
    rstd2 = lax.rsqrt(sumsq * (1.0 / D) + EPS)
    branch_share = jax.nn.sigmoid(branch * rstd2)
    for h in range(2):
        cg = slice(256 * h, 256 * h + 256)
        g_ = r2g[0, :, cg].astype(F32)
        u_ = r2u[0, :, cg].astype(F32)
        for i in range(1, 4):
            g_ = g_ + r2g[i, :, cg].astype(F32)
            u_ = u_ + r2u[i, :, cg].astype(F32)
        g_ = g_ * rstd2
        u_ = u_ * rstd2
        hall[e, :, cg] = (g_ * jax.nn.sigmoid(g_) * u_ * branch_share).astype(BF16)
    over_ep(lambda p: rcopy(hall.at[e], hall.at[e], ssem.at[14], rsem.at[8], p, t).start())

    mark("r_wait_expert")
    for i in (20, 21, 22):
        copies[i].wait()
    for d in range(1, NZ):
        p = lax.rem(z + NZ - d, NZ)
        wait_for(xfull.at[p, :, half(1 - c)], z2sem.at[1, p])

    mark("s_expert")
    def expert_rows(k, carry):
        tot = jnp.zeros((16, 128), F32)
        for m in range(4):
            wide = xfull[k, :, 1024 * m:1024 * m + 1024].astype(F32)
            sq = wide * wide
            for n in range(8):
                tot = tot + sq[:, 128 * n:128 * n + 128]
        scale = lax.rsqrt(jnp.sum(tot, axis=1, keepdims=True) * (1.0 / D) + EPS)
        rows = pl.ds(pl.multiple_of(k * 16, 16), 16)
        for m in range(4):
            cut = slice(1024 * m, 1024 * m + 1024)
            aexp[rows, cut] = (xfull[k, :, cut].astype(F32) * scale * gffn[:, cut]).astype(BF16)
        return carry

    lax.fori_loop(0, NZ, expert_rows, 0)
    acc[...] = jnp.zeros_like(acc)

    def expert_in(k, carry):
        cut = pl.ds(pl.multiple_of(k * 512, 512), 512)
        lhs = aexp[:, cut]
        acc[:, 0:256] += dot(lhs, eg[cut, :])
        acc[:, 256:512] += dot(lhs, eu[cut, :])
        return carry

    lax.fori_loop(0, 8, expert_in, 0)
    g_ = acc[:, 0:256]
    hid = (g_ * jax.nn.sigmoid(g_) * acc[:, 256:512]).astype(BF16)
    aexp[:, 0:256] = hid

    def expert_out(k, carry):
        cut = pl.ds(pl.multiple_of(k * 512, 512), 512)
        prod = dot(aexp[:, 0:256], ed[:, cut]).astype(BF16)
        for n in range(NZ):
            yp[n, :, cut] = prod[16 * n:16 * n + 16]
        return carry

    lax.fori_loop(4 * (1 - c), 4 * (1 - c) + 4, expert_out, 0)
    rcopy(yp.at[:, :, half(1 - c)], yd2d, ssem.at[15], rsem.at[9], e, mate).start()
    lax.fori_loop(4 * c, 4 * c + 4, expert_out, 0)

    mark("r2_pair_sum")
    wait_for(yd2d, rsem.at[9])

    def sum_pair(k, carry):
        both_sum = yp[k, :, half(c)].astype(F32) + yd2d[k].astype(F32)
        ys[0, k] = both_sum[0:8].astype(BF16)
        ys[1, k] = both_sum[8:16].astype(BF16)
        return carry

    lax.fori_loop(0, NZ, sum_pair, 0)

    def back(d, carry):
        j = lax.rem(d + e, NZ)
        pe = c * NZ + j
        rcopy(ys.at[1 - c, :, :, cols(j)], yin.at[:, e], ssem.at[18], rsem.at[12], pe, mate).start()

        @pl.when(pe != e)
        def _():
            rcopy(ys.at[c, :, :, cols(j)], yin.at[:, e], ssem.at[19], rsem.at[12], pe, t).start()

        @pl.when(pe == e)
        def _():
            yin[:, e] = ys[c, :, :, cols(j)]

        return carry

    lax.fori_loop(0, NZ, back, 0)

    mark("t_wait_hidden")
    copies[19].wait()
    wait_for(hall.at[0:15], rsem.at[8])
    mark("u_down")

    def dense_down(g, carry):
        block = jnp.concatenate([hall[4 * g + j] for j in range(4)], axis=0)
        prod = dot(block, dd[...])
        for j in range(4):
            part2[2 * g + j // 2, j % 2] = prod[32 * j:32 * j + 32].astype(BF16)
        return carry

    lax.fori_loop(0, 4, dense_down, 0)
    rcopy(part2.at[:, 1 - c], pd2d2, ssem.at[16], rsem.at[10], e, mate).start()
    mark("v_wait_back")
    either(e // NZ == c, yin.at[:, 0:15], yin, rsem.at[12])
    wait_for(pd2d2, rsem.at[10])
    mark("w_combine")

    def combine(k, carry):
        rows = yin[k].astype(F32).reshape(128, COLS).astype(BF16)
        tot = dot(wtab[k, 0], rows) + dot(wtab[k, 1], rows)
        rsend2[k] = (tot + part2[k, c].astype(F32) + pd2d2[k].astype(F32)).astype(BF16)
        return carry

    lax.fori_loop(0, NZ, combine, 0)
    over_z(lambda p: rcopy(rsend2.at[p], rrecv2.at[z], ssem.at[17], rsem.at[11], e, 2 * p + c).start())
    rrecv2[z] = rsend2[z]
    mark("x_wait_rs")
    wait_for(rrecv2.at[0:7], rsem.at[11])
    tot = resall[z, c].astype(F32)
    for k in range(NZ):
        tot = tot + rrecv2[k].astype(F32)
    outv[...] = tot.astype(BF16)

    mark("z_deliver")
    def deliver(d, carry):
        p = lax.rem(z + d, NZ)

        @pl.when(jnp.logical_or(t != e, p != z))
        def _():
            rcopy(outv, ofull.at[e], ssem.at[20], osem.at[e], t, 2 * p + c).start()

        return carry

    lax.fori_loop(0, NZ, deliver, 0)

    @pl.when(t == e)
    def _():
        ofull[e] = outv[...]

    first = c == lax.rem(e, 2)

    @pl.when(first)
    def _():
        def pass_on(d, carry):
            p = down(d)

            @pl.when(jnp.logical_or(t != e, p != e))
            def _():
                wait_for(ofull.at[p], osem.at[p])

            rcopy(ofull.at[p], out_h.at[:, cols(p)], ssem.at[22], rsem.at[14], e, mate).start()
            pltpu.make_async_copy(ofull.at[p], out_h.at[:, cols(p)], store_sem.at[3]).start()
            return carry

        lax.fori_loop(0, N, pass_on, 0)
        wait_for(ofull, store_sem.at[3])
        wait_for(ofull, ssem.at[22])

    @pl.when(jnp.logical_not(first))
    def _():
        wait_for(out_h, rsem.at[14])

    mark("zz_end")
    wait_for(xall.at[0:15], ssem.at[0])
    wait_for(rtall.at[0:15], ssem.at[1])
    wait_for(csend.at[0:15], ssem.at[2])
    wait_for(heads.at[:, 0:15 * HD], ssem.at[3])
    wait_for(mhall.at[0:15], ssem.at[23])
    wait_for(wp, ssem.at[4])
    wait_for(wpall.at[0:7 * HD], ssem.at[5])
    wait_for(resall.at[0, 0], ssem.at[6])
    wait_for(rsend2.at[0:7], ssem.at[7])
    wait_for(xs.at[0:15], ssem.at[8])
    wait_for(rsend2.at[0:7], ssem.at[9])
    wait_for(yd2d.at[0:7], ssem.at[10])
    for i, ref in ((11, dsg), (24, dsu), (25, d2g), (26, d2u)):
        wait_for(ref.at[0:3], ssem.at[i])
    wait_for(strecv.at[0:15], ssem.at[12])
    wait_for(yd2d.at[0:7], ssem.at[13])
    wait_for(hall.at[0:15], ssem.at[14])
    wait_for(yd2d, ssem.at[15])
    wait_for(pd2d2, ssem.at[16])
    wait_for(rsend2.at[0:7], ssem.at[17])
    wait_for(yin.at[:, 0:8], ssem.at[18])
    either(e // NZ == c, yin.at[:, 0:7], yin.at[:, 0:8], ssem.at[19])
    either(t == e, rsend2.at[0:7], rsend2, ssem.at[20])
    wait_for(wpall.at[0:7 * HD], ssem.at[21])
    for store in stores:
        store.wait()
    mark(None)


def finish_kernel(out_a, nm_a, nn_a, nmax_a, out_o, nm_o, nn_o, nmax_o, out_v, nm_v, nn_v, nmax_v, in_sem, out_sem):
    trips = [(nm_a.at[8 * k:8 * k + 8], nm_v.at[8 * k:8 * k + 8], nm_o.at[8 * k:8 * k + 8]) for k in range(4)]
    trips += [(out_a, out_v, out_o), (nn_a, nn_v, nn_o), (nmax_a, nmax_v, nmax_o)]
    ins = [pltpu.make_async_copy(a, v, in_sem.at[i]) for i, (a, v, _) in enumerate(trips)]
    outs = [pltpu.make_async_copy(v, o, out_sem.at[i]) for i, (_, v, o) in enumerate(trips)]
    for copy in ins:
        copy.start()
    for got, put in zip(ins, outs):
        got.wait()
        put.start()
    for put in outs:
        put.wait()


def on_device(
    tokens, state_matrix, state_norm, state_max, mixer_gain, w_query, w_key, w_value, w_outgate, w_ingate, w_forget,
    forget_bias, w_proj, ffn_gain, w_branch, routes, route_weight, expert_gate, expert_up, expert_down,
    dense_gate, dense_up, dense_down,
):
    any_ = pl.BlockSpec(memory_space=pl.ANY)
    vm = pltpu.VMEM
    scratch = [
        vm((ROWS, D), BF16), vm((ROWS, HD, HD), F32), vm((ROWS, HD), F32), vm((1, ROWS), F32), vm((1, D), F32),
        vm((COLS, 512), BF16), vm((N, D), BF16), vm((N, D), BF16), vm((1, N), F32), vm((HD, COLS), BF16),
        vm((1, D), F32), vm((ROWS, HD), BF16), vm((2, ROWS), jnp.int32), vm((2, ROWS), F32),
        vm((D, COLS), BF16), vm((D, COLS), BF16), vm((COLS, D), BF16), vm((COLS, 1024), BF16), vm((512, COLS), BF16),
        vm((N, ROWS, COLS), BF16), vm((N, ROWS, 512), BF16), vm((N, ROWS, 512), BF16), vm((N, ROWS, HD), BF16),
        vm((ROWS, HALF), BF16), vm((ROWS, HD), F32),
        vm((HALF, COLS), BF16), vm((NZ, 2, ROWS, HD), BF16), vm((NZ, 2, ROWS, COLS), BF16),
        vm((NZ, 2, ROWS, COLS), BF16), vm((NZ, ROWS, COLS), BF16), vm((NZ, ROWS, COLS), BF16),
        vm((NZ, ROWS, COLS), BF16),
        vm((8, 128), F32), vm((N, 8, 128), F32),
        vm((4, 4, ROWS, 512), BF16), vm((4, 4, ROWS, 512), BF16), vm((4, 4, ROWS, 512), BF16),
        vm((4, 4, ROWS, 512), BF16), vm((4, ROWS, 512), BF16), vm((4, ROWS, 512), BF16), vm((4, ROWS, 512), BF16),
        vm((4, ROWS, 512), BF16),
        vm((4, 8, 128), F32), vm((N, 8, 128), F32), vm((N, ROWS, 512), BF16), vm((512, COLS), BF16),
        vm((512, COLS), BF16),
        vm((N, 16, COLS), BF16), vm((NZ, 16, D), BF16), vm((128, D), BF16), vm((128, 512), F32),
        vm((NZ, 16, D), BF16), vm((NZ, 16, HALF), BF16), vm((2, NZ, 8, HALF), BF16), vm((NZ, N, 8, COLS), BF16),
        vm((ROWS, COLS), BF16), vm((N, ROWS, COLS), BF16), vm((ROWS, HD), F32), vm((1, ROWS), F32),
        pltpu.SemaphoreType.DMA((23,)), pltpu.SemaphoreType.DMA((27,)), pltpu.SemaphoreType.DMA((N,)),
        pltpu.SemaphoreType.DMA((15,)), pltpu.SemaphoreType.DMA((3, NZ)), pltpu.SemaphoreType.DMA((3, NZ)),
        pltpu.SemaphoreType.DMA((N,)), pltpu.SemaphoreType.DMA((N,)), pltpu.SemaphoreType.DMA((4,)),
        pltpu.SemaphoreType.DMA((4,)),
    ]
    shapes = (
        jax.ShapeDtypeStruct((ROWS, D), BF16),
        jax.ShapeDtypeStruct((ROWS, HD, HD), F32),
        jax.ShapeDtypeStruct((ROWS, HD), F32),
        jax.ShapeDtypeStruct((1, ROWS), F32),
    )
    results = pl.pallas_call(
        layer_kernel,
        out_shape=shapes,
        in_specs=[any_] * 23,
        out_specs=(any_,) * 4,
        scratch_shapes=scratch,
        compiler_params=pltpu.CompilerParams(
            collective_id=0, has_side_effects=True, vmem_limit_bytes=60 * 1024 * 1024
        ),
        name="layer",
    )(
        tokens, state_matrix.reshape(ROWS, HD, HD), state_norm.reshape(ROWS, HD), state_max.T,
        mixer_gain.reshape(1, D), w_query, w_key, w_value, w_outgate, w_ingate.T, w_forget.T,
        forget_bias.reshape(1, N), w_proj, ffn_gain.reshape(1, D), w_branch.reshape(ROWS, HD), routes.T,
        route_weight.T, expert_gate, expert_up, expert_down, dense_gate, dense_up, dense_down,
    )
    out, nm, nn, nmax = pl.pallas_call(
        finish_kernel,
        out_shape=shapes,
        in_specs=[any_] * 4,
        out_specs=(any_,) * 4,
        scratch_shapes=[vm(shape.shape, shape.dtype) for shape in shapes]
        + [pltpu.SemaphoreType.DMA((7,)), pltpu.SemaphoreType.DMA((7,))],
        name="finish",
    )(*results)
    return (
        out, nm.reshape(ROWS, 1, HD, HD), nn.reshape(ROWS, 1, HD), nmax.T,
    )


def solution(mesh):
    in_specs = (
        P("ep", None), P("ep", "tp", None, None), P("ep", "tp", None), P("ep", "tp"), P(),
        P("ep", "tp"), P("ep", "tp"), P("ep", "tp"), P("ep", "tp"), P(), P(), P(), P("tp", "ep"), P(), P(),
        P("ep", None), P("ep", None), P("ep", None, "tp"), P("ep", None, "tp"), P("ep", "tp", None),
        P("ep", "tp"), P("ep", "tp"), P("tp", "ep"),
    )
    out_specs = (P("ep", None), P("ep", "tp", None, None), P("ep", "tp", None), P("ep", "tp"))
    return jax.shard_map(on_device, mesh=mesh, in_specs=in_specs, out_specs=out_specs, check_vma=False)
```

```python
import functools

import jax
import jax.numpy as jnp
from jax import lax
from jax.experimental import pallas as pl
from jax.experimental.pallas import tpu as pltpu
from jax.sharding import PartitionSpec as P

EPS = 1e-06
MESH = pl.DeviceIdType.MESH
F32 = jnp.float32
BF16 = jnp.bfloat16
N = 16
NZ = 8
ROWS = 32
D = 4096
COLS = 256
HALF = 2048
HD = 128
SECOND_AT = 1
HOPS = (0, 1, 2, 1)
EP_ORDER = sorted(
    [(dy, dx) for dy in range(4) for dx in range(4) if dy + dx], key=lambda o: -(HOPS[o[0]] + HOPS[o[1]])
)
Z_ORDER = (4, 3, 5, 2, 6, 1, 7)


def dot(a, b):
    return jnp.dot(a, b, preferred_element_type=F32)


def dot_rows(a, b):
    return lax.dot_general(a, b, (((1,), (1,)), ((), ())), preferred_element_type=F32)


def layer_kernel(
    tok_h, st_h, sn_h, smax_h, gmix_h, wq_h, wk_h, wv_h, wo_h, wi_h, wf_h, fb_h, wp_h, gffn_h, wbr_h,
    rt_h, rw_h, eg_h, eu_h, ed_h, dg_h, du_h, dd_h,
    out_h, nm_h, nn_h, nmax_h,
    tok, st, sn, smax, gmix, wq, wi, wf, fb, wp, gffn, wbr, rt, rw, eg, eu, ed, dgu, dd,
    xall, csend, crecv, mhall, heads, num,
    wpall, wtab, resall,
    part2, pd2d2, rsend2, rrecv2,
    rtsend, rtall, dsg, dsu, r1g, r1u, d2g, d2u, r2g, r2u, stsend, strecv, halla, hallb, r2all, aall,
    xsa, xsb, xfa, xfb, aexp, acc, yp, yd2d, ys, yin, outv, ofull, nnv, nmaxv,
    load_sem, ssem, bsem, rsem, zsem, z2sem, osem, hsem, gsem, dsem, lsem, store_sem,
):
    e = lax.axis_index("ep")
    t = lax.axis_index("tp")
    z = t // 2
    c = lax.rem(t, 2)
    mate = 2 * z + 1 - c
    ey, ex_ = e // 4, lax.rem(e, 4)

    def rcopy(src, dst, send, recv, pe, pt):
        return pltpu.make_async_remote_copy(
            src_ref=src, dst_ref=dst, send_sem=send, recv_sem=recv, device_id=(pe, pt), device_id_type=MESH
        )

    def wait_for(ref, sem):
        pltpu.make_async_copy(ref, ref, sem).wait()

    def either(less, ref_less, ref_all, sem):
        @pl.when(less)
        def _():
            wait_for(ref_less, sem)

        @pl.when(jnp.logical_not(less))
        def _():
            wait_for(ref_all, sem)

    def ahead(offset):
        return 4 * lax.rem(ey + offset[0], 4) + lax.rem(ex_ + offset[1], 4)

    def behind(offset):
        return 4 * lax.rem(ey + 4 - offset[0], 4) + lax.rem(ex_ + 4 - offset[1], 4)

    def down(d):
        return lax.rem(e + N - d, N)

    def over_ep(fn):
        for offset in EP_ORDER:
            fn(ahead(offset))

    def over_z(fn):
        for d in Z_ORDER:
            fn(lax.rem(z + d, NZ))

    def cols(index):
        return pl.ds(pl.multiple_of(index * COLS, COLS), COLS)

    def half(index):
        return pl.ds(pl.multiple_of(index * HALF, HALF), HALF)

    scopes = []

    def mark(name):
        if scopes:
            scopes.pop().__exit__(None, None, None)
        if name:
            scopes.append(jax.named_scope(name))
            scopes[-1].__enter__()

    mark("a_barrier")
    loads = [
        (tok_h, tok), (gmix_h, gmix),
        (wq_h, wq.at[:, 0:128]), (wk_h, wq.at[:, 128:256]), (wv_h, wq.at[:, 256:384]), (wo_h, wq.at[:, 384:512]),
        (wi_h, wi), (wf_h, wf), (fb_h, fb), (smax_h, smax), (sn_h, sn), (st_h, st), (wp_h, wp), (gffn_h, gffn),
        (wbr_h, wbr), (rt_h, rt), (rw_h, rw), (dg_h, dgu.at[:, 0:512]), (du_h, dgu.at[:, 512:1024]), (dd_h, dd),
        (eg_h.at[0], eg), (eu_h.at[0], eu), (ed_h.at[0], ed),
    ]
    copies = [pltpu.make_async_copy(s, d, load_sem.at[i]) for i, (s, d) in enumerate(loads)]
    for copy in copies:
        copy.start()

    barrier = pltpu.get_barrier_semaphore()

    def greet_ep(p):
        pl.semaphore_signal(barrier, inc=1, device_id=(p, t), device_id_type=MESH)

    def greet_tp(d, carry):
        pl.semaphore_signal(barrier, inc=1, device_id=(e, lax.rem(t + d, N)), device_id_type=MESH)
        return carry

    over_ep(greet_ep)
    lax.fori_loop(1, N, greet_tp, 0)
    copies[0].wait()
    copies[1].wait()
    pl.semaphore_wait(barrier, 2 * (N - 1))

    mark("b_spread_gates")
    over_ep(lambda p: rcopy(tok.at[:, cols(p)], xall.at[e], ssem.at[0], bsem.at[e], p, t).start())
    copies[12].wait()
    mine_wp = wpall.at[pl.ds(pl.multiple_of(t * HD, HD), HD), :]
    rcopy(wp, mine_wp, ssem.at[4], z2sem.at[2, z], e, mate).start()
    over_z(lambda p: rcopy(wp, mine_wp, ssem.at[5], zsem.at[2, z], e, 2 * p + c).start())
    wpall[pl.ds(pl.multiple_of(t * HD, HD), HD), :] = wp[...]
    xall[e] = tok[:, cols(e)]
    gain_e = gmix[:, cols(e)]

    total = jnp.zeros((ROWS, 128), F32)
    for k in range(8):
        wide = tok[:, k * 512:(k + 1) * 512].astype(F32)
        sq = wide * wide
        total = total + (sq[:, 0:128] + sq[:, 128:256]) + (sq[:, 256:384] + sq[:, 384:512])
    rstd = lax.rsqrt(jnp.sum(total, axis=1, keepdims=True) * (1.0 / D) + EPS)
    for i in (6, 7, 8, 9, 15, 16):
        copies[i].wait()
    gi = jnp.zeros((ROWS, N), F32)
    gf = jnp.zeros((ROWS, N), F32)
    for k in range(8):
        cut = slice(k * 512, (k + 1) * 512)
        nb = (tok[:, cut].astype(F32) * rstd * gmix[:, cut]).astype(BF16)
        gi = gi + dot_rows(nb, wi[:, cut])
        gf = gf + dot_rows(nb, wf[:, cut])
    gf = gf + fb[...]
    mine = lax.broadcasted_iota(jnp.int32, (ROWS, N), 1) == t
    gate_in = jnp.sum(jnp.where(mine, gi, 0.0), axis=1, keepdims=True)
    gate_f = jnp.sum(jnp.where(mine, gf, 0.0), axis=1, keepdims=True)
    log_keep = jnp.minimum(gate_f, 0.0) - jnp.log1p(jnp.exp(-jnp.abs(gate_f)))
    square = lax.broadcasted_iota(jnp.int32, (ROWS, ROWS), 0) == lax.broadcasted_iota(jnp.int32, (ROWS, ROWS), 1)
    kept = log_keep + jnp.sum(jnp.where(square, smax[...], 0.0), axis=1, keepdims=True)
    new_max = jnp.maximum(kept, gate_in)
    keep = jnp.exp(kept - new_max)
    write = jnp.exp(gate_in - new_max)
    nmaxv[...] = jnp.sum(jnp.where(square, new_max, 0.0), axis=0, keepdims=True)
    rtsend[...] = jnp.full((8, 128), -1.0, F32)
    rtsend[0:2, 0:ROWS] = rt[...].astype(F32)
    rtsend[2:4, 0:ROWS] = rw[...]
    over_ep(lambda p: rcopy(rtsend, rtall.at[e], ssem.at[1], rsem.at[0], p, t).start())
    rtall[e] = rtsend[...]
    for i in (2, 3, 4, 5, 10, 11):
        copies[i].wait()

    mark("c_qkvo_part")
    for g in range(4):
        ps = [e if 4 * g + j == 0 else behind(EP_ORDER[4 * g + j - 1]) for j in range(4)]
        for j in range(4):
            if 4 * g + j:
                wait_for(xall.at[ps[j]], bsem.at[ps[j]])
        block = jnp.concatenate([xall[p] for p in ps], axis=0)
        prod = dot((block.astype(F32) * gain_e).astype(BF16), wq[...])
        for j in range(4):
            piece = prod[32 * j:32 * j + 32].astype(BF16)
            if 4 * g + j:
                csend[ps[j]] = piece
                rcopy(csend.at[ps[j]], crecv.at[e], ssem.at[2], rsem.at[1], ps[j], t).start()
            else:
                crecv[e] = piece
    mark("d_wait_qkvo")
    wait_for(crecv.at[0:15], rsem.at[1])
    mark("e_cell")
    qkvo = crecv[0].astype(F32)
    for i in range(1, N):
        qkvo = qkvo + crecv[i].astype(F32)
    qkvo = qkvo * rstd
    q = qkvo[:, 0:128]
    kw = qkvo[:, 128:256] * (HD ** -0.5) * write
    v = qkvo[:, 256:384]
    keep_w = jnp.broadcast_to(keep, (ROWS, HD))
    new_norm = keep_w * sn[...] + kw
    nnv[...] = new_norm
    kw_t = jnp.transpose(kw)
    q_t = jnp.transpose(q)
    for b in range(ROWS):
        new = keep_w[b:b + 1, :] * st[b] + kw_t[:, b:b + 1] * v[b:b + 1, :]
        st[b] = new
        num[b:b + 1, :] = jnp.sum(q_t[:, b:b + 1] * new, axis=0, keepdims=True)
    denom = jnp.maximum(jnp.abs(jnp.sum(q * new_norm, axis=1, keepdims=True)), 1.0)
    mhall[e] = (jax.nn.sigmoid(qkvo[:, 384:512]) * (num[...] / denom)).astype(BF16)
    over_ep(lambda p: rcopy(mhall.at[e], mhall.at[e], ssem.at[23], hsem.at[e], p, t).start())
    head_cols = pl.ds(pl.multiple_of(t * HD, HD), HD)

    def turn_heads(p):
        @pl.when(p != t)
        def _():
            rcopy(mhall.at[p], heads.at[:, head_cols], ssem.at[3], rsem.at[2], e, p).start()

        @pl.when(p == t)
        def _():
            heads[:, head_cols] = mhall[p]

    stores = [
        pltpu.make_async_copy(st, nm_h, store_sem.at[0]),
        pltpu.make_async_copy(nnv, nn_h, store_sem.at[1]),
        pltpu.make_async_copy(nmaxv, nmax_h, store_sem.at[2]),
    ]
    for store in stores:
        store.start()

    mark("f_tables")
    wait_for(rtall.at[0:15], rsem.at[0])
    before = (lax.broadcasted_iota(jnp.int32, (128, 128), 0) < lax.broadcasted_iota(jnp.int32, (128, 128), 1)).astype(BF16)
    row8 = lax.broadcasted_iota(jnp.int32, (128, 128), 0)
    row_e = (row8 // 8).astype(F32)
    row16 = lax.broadcasted_iota(jnp.int32, (256, 128), 0)
    row16_e = (row16 // 16).astype(F32)
    row16_q = lax.rem(row16, 16)

    def pick_table(group, low):
        info = rtall[group]
        hit = jnp.logical_or(info[0:1, :] == row16_e, info[1:2, :] == row16_e).astype(F32)
        slot = dot(hit.astype(BF16), before)
        inside = jnp.logical_and(row16_q >= low, row16_q < low + 6)
        fits = jnp.logical_and(slot == (row16_q - low).astype(F32), inside).astype(F32)
        return (hit * fits)[:, 0:ROWS].astype(BF16)

    row_s = lax.rem(row8, 8).astype(F32)

    def table(group):
        info = rtall[group]
        first = (info[0:1, :] == row_e).astype(F32)
        second = (info[1:2, :] == row_e).astype(F32)
        slot = dot((first + second).astype(BF16), before)
        fits = (slot == row_s).astype(F32)
        share = 1.0 / (info[2:3, :] + info[3:4, :])
        weigh = (first * (info[2:3, :] * share) + second * (info[3:4, :] * share)) * fits
        return weigh

    pick0 = pick_table(2 * z, 0)
    pick1 = pick_table(2 * z + 1, 6)

    def wp_rows(index):
        return wpall.at[pl.ds(pl.multiple_of(index * HD, HD), HD), :]

    for d in Z_ORDER:
        p = lax.rem(z + NZ - d, NZ)
        wait_for(wp_rows(2 * p + c), zsem.at[2, p])
        rcopy(wp_rows(2 * p + c), wp_rows(2 * p + c), ssem.at[21], z2sem.at[2, p], e, mate).start()
    turn_heads(e)
    for offset in EP_ORDER:
        p = behind(offset)
        wait_for(mhall.at[p], hsem.at[p])
        turn_heads(p)
    mark("g_wait_heads")
    def combine_table(k, carry):
        turned = jnp.transpose(table(2 * k + c))[0:ROWS, :]
        high = turned.astype(BF16)
        low = (turned - high.astype(F32)).astype(BF16)
        m = lax.rem(k, 4)
        r = lax.broadcasted_iota(jnp.int32, (128, 384), 0)
        q = lax.broadcasted_iota(jnp.int32, (128, 384), 1)
        same = jnp.logical_and(r // 8 == q // 24, lax.rem(q, 24) == 6 * m + lax.rem(r, 8))
        move = jnp.logical_and(same, lax.rem(r, 8) < 6).astype(F32).astype(BF16)
        moved = dot(jnp.concatenate([high, low], axis=0), move).astype(BF16)
        rows = pl.ds(pl.multiple_of(m * ROWS, ROWS), ROWS)
        wtab[k // 4, 0, rows, :] = moved[0:ROWS]
        wtab[k // 4, 1, rows, :] = moved[ROWS:2 * ROWS]
        return carry

    lax.fori_loop(0, NZ, combine_table, 0)
    rr = lax.broadcasted_iota(jnp.int32, (96, 128), 0)
    rq = lax.broadcasted_iota(jnp.int32, (96, 128), 1)
    rest = lax.rem(rr, 48)
    keep_rows = (rq == 16 * (rest // 6) + lax.rem(rest, 6) + 6 * (rr // 48)).astype(F32).astype(BF16)

    for d in range(NZ):
        p = lax.rem(z + NZ - d, NZ)
        wait_for(wp_rows(2 * p + 1 - c), z2sem.at[2, p])

    wait_for(heads.at[:, 0:15 * HD], rsem.at[2])
    mark("h_proj")
    mix = dot(heads[...], wpall[...])
    res_own = (xall[t].astype(F32) + mix).astype(BF16)
    resall[z, c] = res_own

    mark("j_ag_send")
    rcopy(resall.at[z, c], resall.at[z, c], ssem.at[6], z2sem.at[0, z], e, mate).start()
    over_z(lambda p: rcopy(resall.at[z, c], resall.at[z, c], ssem.at[7], zsem.at[0, z], e, 2 * p + c).start())
    mark("k_wait_mate_dispatch")
    wait_for(resall.at[z, 1 - c], z2sem.at[0, z])
    routed = dot(pick0, resall[z, 0]) + dot(pick1, resall[z, 1])
    for ex in range(N):
        xsa[ex] = routed[16 * ex:16 * ex + 8].astype(BF16)
        xsb[ex] = routed[16 * ex + 8:16 * ex + 12].astype(BF16)
    over_ep(lambda p: rcopy(xsa.at[p], xfa.at[z, :, cols(e)], ssem.at[8], rsem.at[5], p, t).start())
    over_ep(lambda p: rcopy(xsb.at[p], xfb.at[z, :, cols(e)], ssem.at[27], rsem.at[15], p, t).start())
    xfa[z, :, cols(e)] = xsa[e]
    xfb[z, :, cols(e)] = xsb[e]

    for i in (13, 14, 17, 18):
        copies[i].wait()
    mark("l_ag_forward")
    gain_f = gffn[:, cols(e)]
    sub = lax.broadcasted_iota(jnp.int32, (ROWS, HD), 0)
    w_rows = wbr[...].astype(F32)
    w_b = jnp.concatenate(
        [jnp.sum(jnp.where(sub == 2 * e + k, w_rows, 0.0), axis=0, keepdims=True) for k in range(2)], axis=1
    ).astype(BF16)

    for d in Z_ORDER:
        p = lax.rem(z + NZ - d, NZ)
        wait_for(resall.at[p, c], zsem.at[0, p])
        rcopy(resall.at[p, c], resall.at[p, c], ssem.at[9], z2sem.at[0, p], e, mate).start()

    mark("n_wait_fwd_dense")
    for d in Z_ORDER:
        p = lax.rem(z + NZ - d, NZ)
        wait_for(resall.at[p, 1 - c], z2sem.at[0, p])
    for k in range(NZ):
        wide = jnp.concatenate([resall[k, 0], resall[k, 1]], axis=0).astype(F32)
        r2all[64 * k:64 * k + 64] = (wide * wide).astype(BF16)
        aall[64 * k:64 * k + 64] = (wide * gain_f).astype(BF16)
    def dense_up(i, carry):
        g = lax.rem(ey + 1 + i, 4)
        rows = pl.ds(pl.multiple_of(g * 128, 128), 128)
        prod = dot(aall[rows, :], dgu[:, 512:1024])
        for j in range(4):
            dsu[g, j] = prod[32 * j:32 * j + 32].astype(BF16)

        @pl.when(g != ey)
        def _():
            rcopy(dsu.at[g], r1u.at[ey], ssem.at[24], gsem.at[1], 4 * g + ex_, t).start()

        return carry

    def dense_gate(g, carry):
        rows = pl.ds(pl.multiple_of(g * 128, 128), 128)
        prod = dot(aall[rows, :], dgu[:, 0:512])
        for j in range(4):
            dsg[j, g] = prod[32 * j:32 * j + 32].astype(BF16)
        return carry

    def dense_stats(g, carry):
        rows = pl.ds(pl.multiple_of(g * 128, 128), 128)
        stat = dot_rows(jnp.ones((8, COLS), BF16), r2all[rows, :])
        br = dot_rows(jnp.broadcast_to(w_b, (8, COLS)), aall[rows, :])
        sub8 = lax.broadcasted_iota(jnp.int32, (8, 128), 0)
        stsend[g] = jnp.where(sub8 < 4, stat, br)
        return carry

    lax.fori_loop(0, 4, dense_up, 0)
    lax.fori_loop(0, 4, dense_gate, 0)
    for d in (2, 1, 3):
        px = lax.rem(ex_ + d, 4)
        rcopy(dsg.at[px], r1g.at[ex_], ssem.at[11], gsem.at[0], 4 * ey + px, t).start()
    mark("m_wait_dispatch")
    wait_for(xsa.at[0:15], rsem.at[5])
    wait_for(xsb.at[0:15], rsem.at[15])

    def to_z(p):
        for ref, i, k in ((xfa, 10, 1), (xfb, 28, 3)):
            part_ = ref.at[z, :, half(c)]
            rcopy(part_, part_, ssem.at[i], zsem.at[k, z], e, 2 * p + c).start()

    over_z(to_z)
    lax.fori_loop(0, 4, dense_stats, 0)
    over_ep(lambda p: rcopy(stsend.at[p // 4], strecv.at[e], ssem.at[12], rsem.at[7], p, t).start())
    r1g[ex_] = dsg[ex_]
    r1u[ey] = dsu[ey]
    strecv[e] = stsend[e // 4]

    mark("o_expert_fwd")
    def second_stage():
        for parts, got, mine, left, sem in ((r1g, d2g, ey, r2g, 0), (r1u, d2u, ex_, r2u, 1)):
            wait_for(parts.at[0:3], gsem.at[sem])
            for k in range(4):
                tot = parts[0, k].astype(F32) + parts[1, k].astype(F32)
                got[k] = (tot + parts[2, k].astype(F32) + parts[3, k].astype(F32)).astype(BF16)
            left[mine] = got[mine]
            for d in (2, 1, 3):
                other = lax.rem(mine + d, 4)
                target = 4 * other + ex_ if sem == 0 else 4 * ey + other
                rcopy(got.at[other], left.at[mine], ssem.at[25 + sem], gsem.at[2 + sem], target, t).start()

    for d in Z_ORDER:
        p = lax.rem(z + NZ - d, NZ)
        for ref, i, k in ((xfa, 13, 1), (xfb, 29, 3)):
            part_ = ref.at[p, :, half(c)]
            wait_for(part_, zsem.at[k, p])
            rcopy(part_, part_, ssem.at[i], z2sem.at[k, p], e, mate).start()
        if d == Z_ORDER[SECOND_AT]:
            second_stage()

    mark("p_wait_dense")
    wait_for(r2g.at[0:3], gsem.at[2])
    wait_for(r2u.at[0:3], gsem.at[3])
    wait_for(strecv.at[0:15], rsem.at[7])
    mark("q_hidden")
    stats = strecv[0]
    for i in range(1, N):
        stats = stats + strecv[i]
    lane = lax.broadcasted_iota(jnp.int32, (ROWS, 128), 1)
    at = lane == lax.broadcasted_iota(jnp.int32, (ROWS, 128), 0) + ROWS * lax.rem(e, 4)
    sumsq = jnp.sum(jnp.where(at, stats[0:1, :], 0.0), axis=1, keepdims=True)
    branch = jnp.sum(jnp.where(at, stats[4:5, :], 0.0), axis=1, keepdims=True)
    rstd2 = lax.rsqrt(sumsq * (1.0 / D) + EPS)
    branch_share = jax.nn.sigmoid(branch * rstd2)
    hidden = [None, None]
    for h in range(2):
        cg = slice(256 * h, 256 * h + 256)
        g_ = r2g[0, :, cg].astype(F32)
        u_ = r2u[0, :, cg].astype(F32)
        for i in range(1, 4):
            g_ = g_ + r2g[i, :, cg].astype(F32)
            u_ = u_ + r2u[i, :, cg].astype(F32)
        g_ = g_ * rstd2
        u_ = u_ * rstd2
        hidden[h] = (g_ * jax.nn.sigmoid(g_) * u_ * branch_share).astype(BF16)
    halla[ey, ex_] = hidden[0]
    hallb[ex_, ey] = hidden[1]
    for d in (2, 1, 3):
        px, py = lax.rem(ex_ + d, 4), lax.rem(ey + d, 4)
        rcopy(halla.at[ey, ex_], halla.at[ey, ex_], ssem.at[14], lsem.at[0], 4 * ey + px, t).start()
        rcopy(hallb.at[ex_, ey], hallb.at[ex_, ey], ssem.at[30], lsem.at[1], 4 * py + ex_, t).start()

    mark("r_wait_expert")
    for i in (20, 21, 22):
        copies[i].wait()
    for d in Z_ORDER:
        p = lax.rem(z + NZ - d, NZ)
        wait_for(xfa.at[p, :, half(1 - c)], z2sem.at[1, p])
        wait_for(xfb.at[p, :, half(1 - c)], z2sem.at[3, p])

    mark("s_expert")
    def expert_rows(k, carry):
        tot = jnp.zeros((16, 128), F32)

        def rows_of(cut):
            third = xfb[k, :, cut].astype(F32)
            return jnp.concatenate([xfa[k, :, cut].astype(F32), third, jnp.zeros_like(third)], axis=0)

        for m in range(4):
            wide = rows_of(slice(1024 * m, 1024 * m + 1024))
            sq = wide * wide
            for n in range(8):
                tot = tot + sq[:, 128 * n:128 * n + 128]
        scale = lax.rsqrt(jnp.sum(tot, axis=1, keepdims=True) * (1.0 / D) + EPS)
        rows = pl.ds(pl.multiple_of(k * 16, 16), 16)
        for m in range(4):
            cut = slice(1024 * m, 1024 * m + 1024)
            aexp[rows, cut] = (rows_of(cut) * scale * gffn[:, cut]).astype(BF16)
        return carry

    lax.fori_loop(0, NZ, expert_rows, 0)
    acc[...] = jnp.zeros_like(acc)

    def expert_in(k, carry):
        cut = pl.ds(pl.multiple_of(k * 512, 512), 512)
        lhs = aexp[:, cut]
        acc[:, 0:256] += dot(lhs, eg[cut, :])
        acc[:, 256:512] += dot(lhs, eu[cut, :])
        return carry

    lax.fori_loop(0, 8, expert_in, 0)
    g_ = acc[:, 0:256]
    hid = (g_ * jax.nn.sigmoid(g_) * acc[:, 256:512]).astype(BF16)
    aexp[:, 0:256] = hid

    mark("s3_hidden_stage")
    wait_for(halla.at[0, 0:3], lsem.at[0])
    wait_for(hallb.at[0, 0:3], lsem.at[1])
    for d in (2, 1, 3):
        px, py = lax.rem(ex_ + d, 4), lax.rem(ey + d, 4)
        rcopy(halla.at[ey], halla.at[ey], ssem.at[31], lsem.at[2], 4 * py + ex_, t).start()
        rcopy(hallb.at[ex_], hallb.at[ex_], ssem.at[32], lsem.at[3], 4 * ey + px, t).start()
    mark("s2_expert_out")

    def chunk_of(k):
        return lax.rem(k + e, 4)

    def expert_out(part_, k):
        at_ = pl.ds(pl.multiple_of(part_ * HALF + k * 512, 512), 512)
        return dot(aexp[:, 0:256], ed[:, at_])

    def for_mate(i, carry):
        k = chunk_of(i)
        prod = expert_out(1 - c, k).astype(BF16)
        for n in range(NZ):
            yp[k, n] = prod[16 * n:16 * n + 16]
        rcopy(yp.at[k], yd2d.at[k], ssem.at[15], dsem.at[k], e, mate).start()
        return carry

    def back(j, pe):
        rcopy(ys.at[1 - c, :, :, cols(j)], yin.at[:, e], ssem.at[18], rsem.at[12], pe, mate).start()

        @pl.when(pe != e)
        def _():
            rcopy(ys.at[c, :, :, cols(j)], yin.at[:, e], ssem.at[19], rsem.at[12], pe, t).start()

        @pl.when(pe == e)
        def _():
            yin[:, e] = ys[c, :, :, cols(j)]

    def for_own(i, carry):
        k = chunk_of(i)
        prod = expert_out(c, k)
        at_ = pl.ds(pl.multiple_of(k * 512, 512), 512)
        wait_for(yd2d.at[k], dsem.at[k])
        both_sum = jnp.concatenate([prod[16 * n:16 * n + 16] + yd2d[k, n].astype(F32) for n in range(NZ)], axis=0)
        compact = dot(keep_rows, both_sum.astype(BF16))
        for n in range(4):
            ys[n // 2, n % 2, :, at_] = compact[24 * n:24 * n + 24].astype(BF16)
        for j in range(2):
            back(2 * k + j, c * NZ + 2 * k + j)
        return carry

    lax.fori_loop(0, 4, for_mate, 0)
    lax.fori_loop(0, 4, for_own, 0)

    mark("t_wait_hidden")
    copies[19].wait()
    wait_for(halla.at[0:3], lsem.at[2])
    wait_for(hallb.at[0:3], lsem.at[3])
    mark("u_down")

    def dense_down(g, carry):
        left = jnp.concatenate([halla[g, j] for j in range(4)], axis=0)
        right = jnp.concatenate([hallb[j, g] for j in range(4)], axis=0)
        prod = dot(jnp.concatenate([left, right], axis=1), dd[...])
        for j in range(4):
            part2[2 * g + j // 2, j % 2] = prod[32 * j:32 * j + 32].astype(BF16)
        return carry

    lax.fori_loop(0, 4, dense_down, 0)
    rcopy(part2.at[:, 1 - c], pd2d2, ssem.at[16], rsem.at[10], e, mate).start()
    mark("v_wait_back")
    either(e // NZ == c, yin.at[:, 0:15], yin, rsem.at[12])
    wait_for(pd2d2, rsem.at[10])
    mark("w_combine")

    for g in range(2):
        rows = yin[g].astype(F32).reshape(384, COLS).astype(BF16)
        tot = dot(wtab[g, 0], rows) + dot(wtab[g, 1], rows)
        for m in range(4):
            k = 4 * g + m
            total_ = tot[32 * m:32 * m + 32] + part2[k, c].astype(F32) + pd2d2[k].astype(F32)
            rsend2[k] = total_.astype(BF16)
    over_z(lambda p: rcopy(rsend2.at[p], rrecv2.at[z], ssem.at[17], rsem.at[11], e, 2 * p + c).start())
    rrecv2[z] = rsend2[z]
    mark("x_wait_rs")
    wait_for(rrecv2.at[0:7], rsem.at[11])
    tot = resall[z, c].astype(F32)
    for k in range(NZ):
        tot = tot + rrecv2[k].astype(F32)
    outv[...] = tot.astype(BF16)

    mark("z_deliver")
    def deliver(d):
        p = lax.rem(z + d, NZ)

        @pl.when(jnp.logical_or(t != e, p != z))
        def _():
            rcopy(outv, ofull.at[e], ssem.at[20], osem.at[e], t, 2 * p + c).start()

    for d in Z_ORDER + (0,):
        deliver(d)

    @pl.when(t == e)
    def _():
        ofull[e] = outv[...]

    first = c == lax.rem(e, 2)

    @pl.when(first)
    def _():
        def pass_on(d, carry):
            p = down(d)

            @pl.when(jnp.logical_or(t != e, p != e))
            def _():
                wait_for(ofull.at[p], osem.at[p])

            rcopy(ofull.at[p], out_h.at[:, cols(p)], ssem.at[22], rsem.at[14], e, mate).start()
            pltpu.make_async_copy(ofull.at[p], out_h.at[:, cols(p)], store_sem.at[3]).start()
            return carry

        lax.fori_loop(0, N, pass_on, 0)
        wait_for(ofull, store_sem.at[3])
        wait_for(ofull, ssem.at[22])

    @pl.when(jnp.logical_not(first))
    def _():
        wait_for(out_h, rsem.at[14])

    mark("zz_end")
    wait_for(xall.at[0:15], ssem.at[0])
    wait_for(rtall.at[0:15], ssem.at[1])
    wait_for(csend.at[0:15], ssem.at[2])
    wait_for(heads.at[:, 0:15 * HD], ssem.at[3])
    wait_for(mhall.at[0:15], ssem.at[23])
    wait_for(wp, ssem.at[4])
    wait_for(wpall.at[0:7 * HD], ssem.at[5])
    wait_for(resall.at[0, 0], ssem.at[6])
    wait_for(rsend2.at[0:7], ssem.at[7])
    wait_for(xsa.at[0:15], ssem.at[8])
    wait_for(xsb.at[0:15], ssem.at[27])
    wait_for(rsend2.at[0:7], ssem.at[9])
    wait_for(xfa.at[0:7, :, 0:HALF], ssem.at[10])
    wait_for(xfb.at[0:7, :, 0:HALF], ssem.at[28])
    for i, ref in ((11, dsg), (24, dsu), (25, d2g), (26, d2u)):
        wait_for(ref.at[0:3], ssem.at[i])
    wait_for(strecv.at[0:15], ssem.at[12])
    wait_for(xfa.at[0:7, :, 0:HALF], ssem.at[13])
    wait_for(xfb.at[0:7, :, 0:HALF], ssem.at[29])
    for i, ref in ((14, halla.at[0]), (30, hallb.at[0]), (31, halla), (32, hallb)):
        wait_for(ref.at[0:3], ssem.at[i])
    wait_for(yd2d, ssem.at[15])
    wait_for(pd2d2, ssem.at[16])
    wait_for(rsend2.at[0:7], ssem.at[17])
    wait_for(yin.at[:, 0:8], ssem.at[18])
    either(e // NZ == c, yin.at[:, 0:7], yin.at[:, 0:8], ssem.at[19])
    either(t == e, rsend2.at[0:7], rsend2, ssem.at[20])
    wait_for(wpall.at[0:7 * HD], ssem.at[21])
    for store in stores:
        store.wait()
    mark(None)


def finish_kernel(out_a, nm_a, nn_a, nmax_a, out_o, nm_o, nn_o, nmax_o, out_v, nm_v, nn_v, nmax_v, in_sem, out_sem):
    trips = [(nm_a.at[8 * k:8 * k + 8], nm_v.at[8 * k:8 * k + 8], nm_o.at[8 * k:8 * k + 8]) for k in range(4)]
    trips += [(out_a, out_v, out_o), (nn_a, nn_v, nn_o), (nmax_a, nmax_v, nmax_o)]
    ins = [pltpu.make_async_copy(a, v, in_sem.at[i]) for i, (a, v, _) in enumerate(trips)]
    outs = [pltpu.make_async_copy(v, o, out_sem.at[i]) for i, (_, v, o) in enumerate(trips)]
    for copy in ins:
        copy.start()
    for got, put in zip(ins, outs):
        got.wait()
        put.start()
    for put in outs:
        put.wait()


def on_device(
    tokens, state_matrix, state_norm, state_max, mixer_gain, w_query, w_key, w_value, w_outgate, w_ingate, w_forget,
    forget_bias, w_proj, ffn_gain, w_branch, routes, route_weight, expert_gate, expert_up, expert_down,
    dense_gate, dense_up, dense_down,
):
    any_ = pl.BlockSpec(memory_space=pl.ANY)
    vm = pltpu.VMEM
    scratch = [
        vm((ROWS, D), BF16), vm((ROWS, HD, HD), F32), vm((ROWS, HD), F32), vm((1, ROWS), F32), vm((1, D), F32),
        vm((COLS, 512), BF16), vm((N, D), BF16), vm((N, D), BF16), vm((1, N), F32), vm((HD, COLS), BF16),
        vm((1, D), F32), vm((ROWS, HD), BF16), vm((2, ROWS), jnp.int32), vm((2, ROWS), F32),
        vm((D, COLS), BF16), vm((D, COLS), BF16), vm((COLS, D), BF16), vm((COLS, 1024), BF16), vm((512, COLS), BF16),
        vm((N, ROWS, COLS), BF16), vm((N, ROWS, 512), BF16), vm((N, ROWS, 512), BF16), vm((N, ROWS, HD), BF16),
        vm((ROWS, HALF), BF16), vm((ROWS, HD), F32),
        vm((HALF, COLS), BF16), vm((2, 2, 128, 384), BF16), vm((NZ, 2, ROWS, COLS), BF16),
        vm((NZ, 2, ROWS, COLS), BF16), vm((NZ, ROWS, COLS), BF16), vm((NZ, ROWS, COLS), BF16),
        vm((NZ, ROWS, COLS), BF16),
        vm((8, 128), F32), vm((N, 8, 128), F32),
        vm((4, 4, ROWS, 512), BF16), vm((4, 4, ROWS, 512), BF16), vm((4, 4, ROWS, 512), BF16),
        vm((4, 4, ROWS, 512), BF16), vm((4, ROWS, 512), BF16), vm((4, ROWS, 512), BF16), vm((4, ROWS, 512), BF16),
        vm((4, ROWS, 512), BF16),
        vm((4, 8, 128), F32), vm((N, 8, 128), F32), vm((4, 4, ROWS, COLS), BF16),
        vm((4, 4, ROWS, COLS), BF16), vm((512, COLS), BF16),
        vm((512, COLS), BF16),
        vm((N, 8, COLS), BF16), vm((N, 4, COLS), BF16), vm((NZ, 8, D), BF16), vm((NZ, 4, D), BF16), vm((128, D), BF16), vm((128, 512), F32),
        vm((4, NZ, 16, 512), BF16), vm((4, NZ, 16, 512), BF16), vm((2, 2, 24, HALF), BF16), vm((2, N, 24, COLS), BF16),
        vm((ROWS, COLS), BF16), vm((N, ROWS, COLS), BF16), vm((ROWS, HD), F32), vm((1, ROWS), F32),
        pltpu.SemaphoreType.DMA((23,)), pltpu.SemaphoreType.DMA((33,)), pltpu.SemaphoreType.DMA((N,)),
        pltpu.SemaphoreType.DMA((16,)), pltpu.SemaphoreType.DMA((4, NZ)), pltpu.SemaphoreType.DMA((4, NZ)),
        pltpu.SemaphoreType.DMA((N,)), pltpu.SemaphoreType.DMA((N,)), pltpu.SemaphoreType.DMA((4,)),
        pltpu.SemaphoreType.DMA((4,)), pltpu.SemaphoreType.DMA((4,)), pltpu.SemaphoreType.DMA((4,)),
    ]
    shapes = (
        jax.ShapeDtypeStruct((ROWS, D), BF16),
        jax.ShapeDtypeStruct((ROWS, HD, HD), F32),
        jax.ShapeDtypeStruct((ROWS, HD), F32),
        jax.ShapeDtypeStruct((1, ROWS), F32),
    )
    results = pl.pallas_call(
        layer_kernel,
        out_shape=shapes,
        in_specs=[any_] * 23,
        out_specs=(any_,) * 4,
        scratch_shapes=scratch,
        compiler_params=pltpu.CompilerParams(
            collective_id=0, has_side_effects=True, vmem_limit_bytes=60 * 1024 * 1024
        ),
        name="layer",
    )(
        tokens, state_matrix.reshape(ROWS, HD, HD), state_norm.reshape(ROWS, HD), state_max.T,
        mixer_gain.reshape(1, D), w_query, w_key, w_value, w_outgate, w_ingate.T, w_forget.T,
        forget_bias.reshape(1, N), w_proj, ffn_gain.reshape(1, D), w_branch.reshape(ROWS, HD), routes.T,
        route_weight.T, expert_gate, expert_up, expert_down, dense_gate, dense_up, dense_down,
    )
    out, nm, nn, nmax = pl.pallas_call(
        finish_kernel,
        out_shape=shapes,
        in_specs=[any_] * 4,
        out_specs=(any_,) * 4,
        scratch_shapes=[vm(shape.shape, shape.dtype) for shape in shapes]
        + [pltpu.SemaphoreType.DMA((7,)), pltpu.SemaphoreType.DMA((7,))],
        name="finish",
    )(*results)
    return (
        out, nm.reshape(ROWS, 1, HD, HD), nn.reshape(ROWS, 1, HD), nmax.T,
    )


def solution(mesh):
    in_specs = (
        P("ep", None), P("ep", "tp", None, None), P("ep", "tp", None), P("ep", "tp"), P(),
        P("ep", "tp"), P("ep", "tp"), P("ep", "tp"), P("ep", "tp"), P(), P(), P(), P("tp", "ep"), P(), P(),
        P("ep", None), P("ep", None), P("ep", None, "tp"), P("ep", None, "tp"), P("ep", "tp", None),
        P("ep", "tp"), P("ep", "tp"), P("tp", "ep"),
    )
    out_specs = (P("ep", None), P("ep", "tp", None, None), P("ep", "tp", None), P("ep", "tp"))
    return jax.shard_map(on_device, mesh=mesh, in_specs=in_specs, out_specs=out_specs, check_vma=False)
```

```python
import functools

import jax
import jax.numpy as jnp
from jax import lax
from jax.experimental import pallas as pl
from jax.experimental.pallas import tpu as pltpu
from jax.sharding import PartitionSpec as P

EPS = 1e-06
MESH = pl.DeviceIdType.MESH
F32 = jnp.float32
BF16 = jnp.bfloat16
N = 16
NZ = 8
ROWS = 32
D = 4096
COLS = 256
HALF = 2048
HD = 128
SECOND_AT = 0
HOPS = (0, 1, 2, 1)
EP_ORDER = sorted(
    [(dy, dx) for dy in range(4) for dx in range(4) if dy + dx], key=lambda o: -(HOPS[o[0]] + HOPS[o[1]])
)
Z_ORDER = (4, 3, 5, 2, 6, 1, 7)


def dot(a, b):
    return jnp.dot(a, b, preferred_element_type=F32)


def dot_rows(a, b):
    return lax.dot_general(a, b, (((1,), (1,)), ((), ())), preferred_element_type=F32)


def layer_kernel(
    tok_h, st_h, sn_h, smax_h, gmix_h, wq_h, wk_h, wv_h, wo_h, wi_h, wf_h, fb_h, wp_h, gffn_h, wbr_h,
    rt_h, rw_h, eg_h, eu_h, ed_h, dg_h, du_h, dd_h,
    ofull, nm, nnv, nmaxv,
    tok, st, sn, smax, gmix, wq, wi, wf, fb, wp, gffn, wbr, rt, rw, eg, eu, ed, dgu, dd,
    xall, csend, crecv, mhall, heads, num,
    wpall, wtab, resall,
    part2, pd2d2, rsend2, rrecv2,
    rtsend, rtall, dsg, dsu, r1g, r1u, d2g, d2u, r2g, r2u, stsend, strecv, halla, hallb, r2all, aall,
    xsa, xsb, xfa, xfb, aexp, acc, yp, yd2d, ys, yin, outv,
    load_sem, ssem, bsem, rsem, zsem, z2sem, osem, hsem, gsem, dsem, lsem,
):
    e = lax.axis_index("ep")
    t = lax.axis_index("tp")
    z = t // 2
    c = lax.rem(t, 2)
    mate = 2 * z + 1 - c
    ey, ex_ = e // 4, lax.rem(e, 4)

    def rcopy(src, dst, send, recv, pe, pt):
        return pltpu.make_async_remote_copy(
            src_ref=src, dst_ref=dst, send_sem=send, recv_sem=recv, device_id=(pe, pt), device_id_type=MESH
        )

    def wait_for(ref, sem):
        pltpu.make_async_copy(ref, ref, sem).wait()

    def either(less, ref_less, ref_all, sem):
        @pl.when(less)
        def _():
            wait_for(ref_less, sem)

        @pl.when(jnp.logical_not(less))
        def _():
            wait_for(ref_all, sem)

    def ahead(offset):
        return 4 * lax.rem(ey + offset[0], 4) + lax.rem(ex_ + offset[1], 4)

    def behind(offset):
        return 4 * lax.rem(ey + 4 - offset[0], 4) + lax.rem(ex_ + 4 - offset[1], 4)

    def down(d):
        return lax.rem(e + N - d, N)

    def over_ep(fn):
        for offset in EP_ORDER:
            fn(ahead(offset))

    def over_z(fn):
        for d in Z_ORDER:
            fn(lax.rem(z + d, NZ))

    def cols(index):
        return pl.ds(pl.multiple_of(index * COLS, COLS), COLS)

    def half(index):
        return pl.ds(pl.multiple_of(index * HALF, HALF), HALF)

    scopes = []

    def mark(name):
        if scopes:
            scopes.pop().__exit__(None, None, None)
        if name:
            scopes.append(jax.named_scope(name))
            scopes[-1].__enter__()

    mark("a_barrier")
    loads = [
        (tok_h, tok), (gmix_h, gmix),
        (wq_h, wq.at[:, 0:128]), (wk_h, wq.at[:, 128:256]), (wv_h, wq.at[:, 256:384]), (wo_h, wq.at[:, 384:512]),
        (wi_h, wi), (wf_h, wf), (fb_h, fb), (smax_h, smax), (sn_h, sn), (st_h, st), (wp_h, wp), (gffn_h, gffn),
        (wbr_h, wbr), (rt_h, rt), (rw_h, rw), (dg_h, dgu.at[:, 0:512]), (du_h, dgu.at[:, 512:1024]), (dd_h, dd),
        (eg_h.at[0], eg), (eu_h.at[0], eu), (ed_h.at[0], ed),
    ]
    copies = [pltpu.make_async_copy(s, d, load_sem.at[i]) for i, (s, d) in enumerate(loads)]
    for copy in copies:
        copy.start()

    barrier = pltpu.get_barrier_semaphore()

    def greet_ep(p):
        pl.semaphore_signal(barrier, inc=1, device_id=(p, t), device_id_type=MESH)

    def greet_tp(d, carry):
        pl.semaphore_signal(barrier, inc=1, device_id=(e, lax.rem(t + d, N)), device_id_type=MESH)
        return carry

    over_ep(greet_ep)
    lax.fori_loop(1, N, greet_tp, 0)
    copies[0].wait()
    copies[1].wait()
    pl.semaphore_wait(barrier, 2 * (N - 1))

    mark("b_spread_gates")
    over_ep(lambda p: rcopy(tok.at[:, cols(p)], xall.at[e], ssem.at[0], bsem.at[e], p, t).start())
    copies[12].wait()
    mine_wp = wpall.at[pl.ds(pl.multiple_of(t * HD, HD), HD), :]
    rcopy(wp, mine_wp, ssem.at[4], z2sem.at[2, z], e, mate).start()
    over_z(lambda p: rcopy(wp, mine_wp, ssem.at[5], zsem.at[2, z], e, 2 * p + c).start())
    wpall[pl.ds(pl.multiple_of(t * HD, HD), HD), :] = wp[...]
    xall[e] = tok[:, cols(e)]
    gain_e = gmix[:, cols(e)]

    total = jnp.zeros((ROWS, 128), F32)
    for k in range(8):
        wide = tok[:, k * 512:(k + 1) * 512].astype(F32)
        sq = wide * wide
        total = total + (sq[:, 0:128] + sq[:, 128:256]) + (sq[:, 256:384] + sq[:, 384:512])
    rstd = lax.rsqrt(jnp.sum(total, axis=1, keepdims=True) * (1.0 / D) + EPS)
    for i in (6, 7, 8, 9, 15, 16):
        copies[i].wait()
    gi = jnp.zeros((ROWS, N), F32)
    gf = jnp.zeros((ROWS, N), F32)
    for k in range(8):
        cut = slice(k * 512, (k + 1) * 512)
        nb = (tok[:, cut].astype(F32) * rstd * gmix[:, cut]).astype(BF16)
        gi = gi + dot_rows(nb, wi[:, cut])
        gf = gf + dot_rows(nb, wf[:, cut])
    gf = gf + fb[...]
    mine = lax.broadcasted_iota(jnp.int32, (ROWS, N), 1) == t
    gate_in = jnp.sum(jnp.where(mine, gi, 0.0), axis=1, keepdims=True)
    gate_f = jnp.sum(jnp.where(mine, gf, 0.0), axis=1, keepdims=True)
    log_keep = jnp.minimum(gate_f, 0.0) - jnp.log1p(jnp.exp(-jnp.abs(gate_f)))
    square = lax.broadcasted_iota(jnp.int32, (ROWS, ROWS), 0) == lax.broadcasted_iota(jnp.int32, (ROWS, ROWS), 1)
    kept = log_keep + jnp.sum(jnp.where(square, smax[...], 0.0), axis=1, keepdims=True)
    new_max = jnp.maximum(kept, gate_in)
    keep = jnp.exp(kept - new_max)
    write = jnp.exp(gate_in - new_max)
    nmaxv[...] = jnp.sum(jnp.where(square, new_max, 0.0), axis=0, keepdims=True)
    rtsend[...] = jnp.full((8, 128), -1.0, F32)
    rtsend[0:2, 0:ROWS] = rt[...].astype(F32)
    rtsend[2:4, 0:ROWS] = rw[...]
    over_ep(lambda p: rcopy(rtsend, rtall.at[e], ssem.at[1], rsem.at[0], p, t).start())
    rtall[e] = rtsend[...]
    for i in (2, 3, 4, 5, 10, 11):
        copies[i].wait()

    mark("c_qkvo_part")
    for g in range(4):
        ps = [e if 4 * g + j == 0 else behind(EP_ORDER[4 * g + j - 1]) for j in range(4)]
        for j in range(4):
            if 4 * g + j:
                wait_for(xall.at[ps[j]], bsem.at[ps[j]])
        block = jnp.concatenate([xall[p] for p in ps], axis=0)
        prod = dot((block.astype(F32) * gain_e).astype(BF16), wq[...])
        for j in range(4):
            piece = prod[32 * j:32 * j + 32].astype(BF16)
            if 4 * g + j:
                csend[ps[j]] = piece
                rcopy(csend.at[ps[j]], crecv.at[e], ssem.at[2], rsem.at[1], ps[j], t).start()
            else:
                crecv[e] = piece
    mark("d_wait_qkvo")
    keep_w = jnp.broadcast_to(keep, (ROWS, HD))
    for b in range(ROWS):
        st[b] = keep_w[b:b + 1, :] * st[b]
    wait_for(crecv.at[0:15], rsem.at[1])
    mark("e_cell")
    qkvo = crecv[0].astype(F32)
    for i in range(1, N):
        qkvo = qkvo + crecv[i].astype(F32)
    qkvo = qkvo * rstd
    q = qkvo[:, 0:128]
    kw = qkvo[:, 128:256] * (HD ** -0.5) * write
    v = qkvo[:, 256:384]
    new_norm = keep_w * sn[...] + kw
    nnv[...] = new_norm
    kw_t = jnp.transpose(kw)
    q_t = jnp.transpose(q)
    for b in range(ROWS):
        new = st[b] + kw_t[:, b:b + 1] * v[b:b + 1, :]
        nm[b] = new
        num[b:b + 1, :] = jnp.sum(q_t[:, b:b + 1] * new, axis=0, keepdims=True)
    denom = jnp.maximum(jnp.abs(jnp.sum(q * new_norm, axis=1, keepdims=True)), 1.0)
    mhall[e] = (jax.nn.sigmoid(qkvo[:, 384:512]) * (num[...] / denom)).astype(BF16)
    over_ep(lambda p: rcopy(mhall.at[e], mhall.at[e], ssem.at[23], hsem.at[e], p, t).start())
    head_cols = pl.ds(pl.multiple_of(t * HD, HD), HD)

    def turn_heads(p):
        @pl.when(p != t)
        def _():
            rcopy(mhall.at[p], heads.at[:, head_cols], ssem.at[3], rsem.at[2], e, p).start()

        @pl.when(p == t)
        def _():
            heads[:, head_cols] = mhall[p]

    mark("f_tables")
    wait_for(rtall.at[0:15], rsem.at[0])
    before = (lax.broadcasted_iota(jnp.int32, (128, 128), 0) < lax.broadcasted_iota(jnp.int32, (128, 128), 1)).astype(BF16)
    row8 = lax.broadcasted_iota(jnp.int32, (128, 128), 0)
    row_e = (row8 // 8).astype(F32)
    row16 = lax.broadcasted_iota(jnp.int32, (256, 128), 0)
    row16_e = (row16 // 16).astype(F32)
    row16_q = lax.rem(row16, 16)

    def pick_table(group, low):
        info = rtall[group]
        hit = jnp.logical_or(info[0:1, :] == row16_e, info[1:2, :] == row16_e).astype(F32)
        slot = dot(hit.astype(BF16), before)
        inside = jnp.logical_and(row16_q >= low, row16_q < low + 6)
        fits = jnp.logical_and(slot == (row16_q - low).astype(F32), inside).astype(F32)
        return (hit * fits)[:, 0:ROWS].astype(BF16)

    row_s = lax.rem(row8, 8).astype(F32)

    def table(group):
        info = rtall[group]
        first = (info[0:1, :] == row_e).astype(F32)
        second = (info[1:2, :] == row_e).astype(F32)
        slot = dot((first + second).astype(BF16), before)
        fits = (slot == row_s).astype(F32)
        share = 1.0 / (info[2:3, :] + info[3:4, :])
        weigh = (first * (info[2:3, :] * share) + second * (info[3:4, :] * share)) * fits
        return weigh

    pick0 = pick_table(2 * z, 0)
    pick1 = pick_table(2 * z + 1, 6)

    def wp_rows(index):
        return wpall.at[pl.ds(pl.multiple_of(index * HD, HD), HD), :]

    for d in Z_ORDER:
        p = lax.rem(z + NZ - d, NZ)
        wait_for(wp_rows(2 * p + c), zsem.at[2, p])
        rcopy(wp_rows(2 * p + c), wp_rows(2 * p + c), ssem.at[21], z2sem.at[2, p], e, mate).start()
    turn_heads(e)
    for offset in EP_ORDER:
        p = behind(offset)
        wait_for(mhall.at[p], hsem.at[p])
        turn_heads(p)
    mark("g_wait_heads")
    def combine_table(k, carry):
        turned = jnp.transpose(table(2 * k + c))[0:ROWS, :]
        high = turned.astype(BF16)
        low = (turned - high.astype(F32)).astype(BF16)
        m = lax.rem(k, 4)
        r = lax.broadcasted_iota(jnp.int32, (128, 384), 0)
        q = lax.broadcasted_iota(jnp.int32, (128, 384), 1)
        same = jnp.logical_and(r // 8 == q // 24, lax.rem(q, 24) == 6 * m + lax.rem(r, 8))
        move = jnp.logical_and(same, lax.rem(r, 8) < 6).astype(F32).astype(BF16)
        moved = dot(jnp.concatenate([high, low], axis=0), move).astype(BF16)
        rows = pl.ds(pl.multiple_of(m * ROWS, ROWS), ROWS)
        wtab[k // 4, 0, rows, :] = moved[0:ROWS]
        wtab[k // 4, 1, rows, :] = moved[ROWS:2 * ROWS]
        return carry

    lax.fori_loop(0, NZ, combine_table, 0)
    rr = lax.broadcasted_iota(jnp.int32, (96, 128), 0)
    rq = lax.broadcasted_iota(jnp.int32, (96, 128), 1)
    rest = lax.rem(rr, 48)
    keep_rows = (rq == 16 * (rest // 6) + lax.rem(rest, 6) + 6 * (rr // 48)).astype(F32).astype(BF16)

    for d in range(NZ):
        p = lax.rem(z + NZ - d, NZ)
        wait_for(wp_rows(2 * p + 1 - c), z2sem.at[2, p])

    wait_for(heads.at[:, 0:15 * HD], rsem.at[2])
    mark("h_proj")
    mix = dot(heads[...], wpall[...])
    res_own = (xall[t].astype(F32) + mix).astype(BF16)
    resall[z, c] = res_own

    mark("j_ag_send")
    rcopy(resall.at[z, c], resall.at[z, c], ssem.at[6], z2sem.at[0, z], e, mate).start()
    over_z(lambda p: rcopy(resall.at[z, c], resall.at[z, c], ssem.at[7], zsem.at[0, z], e, 2 * p + c).start())
    mark("k_wait_mate_dispatch")
    wait_for(resall.at[z, 1 - c], z2sem.at[0, z])
    routed = dot(pick0, resall[z, 0]) + dot(pick1, resall[z, 1])
    for ex in range(N):
        xsa[ex] = routed[16 * ex:16 * ex + 8].astype(BF16)
        xsb[ex] = routed[16 * ex + 8:16 * ex + 12].astype(BF16)
    over_ep(lambda p: rcopy(xsa.at[p], xfa.at[z, :, cols(e)], ssem.at[8], rsem.at[5], p, t).start())
    over_ep(lambda p: rcopy(xsb.at[p], xfb.at[z, :, cols(e)], ssem.at[27], rsem.at[15], p, t).start())
    xfa[z, :, cols(e)] = xsa[e]
    xfb[z, :, cols(e)] = xsb[e]

    for i in (13, 14, 17, 18):
        copies[i].wait()
    mark("l_ag_forward")
    gain_f = gffn[:, cols(e)]
    sub = lax.broadcasted_iota(jnp.int32, (ROWS, HD), 0)
    w_rows = wbr[...].astype(F32)
    w_b = jnp.concatenate(
        [jnp.sum(jnp.where(sub == 2 * e + k, w_rows, 0.0), axis=0, keepdims=True) for k in range(2)], axis=1
    ).astype(BF16)

    for d in Z_ORDER:
        p = lax.rem(z + NZ - d, NZ)
        wait_for(resall.at[p, c], zsem.at[0, p])
        rcopy(resall.at[p, c], resall.at[p, c], ssem.at[9], z2sem.at[0, p], e, mate).start()

    mark("n_wait_fwd_dense")
    def rows_for(k, par):
        return pl.ds(pl.multiple_of(64 * k + 32 * par, 32), 32)

    def dense_rows(par):
        for k in range(NZ):
            wide = resall[k, par].astype(F32)
            r2all[rows_for(k, par), :] = (wide * wide).astype(BF16)
            aall[rows_for(k, par), :] = (wide * gain_f).astype(BF16)

    def dense_part(i, par, upper):
        lhs = jnp.concatenate([aall[rows_for(4 * i + j, par), :] for j in range(4)], axis=0)
        prod = dot(lhs, dgu[:, 512:1024] if upper else dgu[:, 0:512])
        for j in range(4):
            piece = prod[32 * j:32 * j + 32].astype(BF16)
            py, px = 2 * i + j // 2, 2 * (j % 2) + par
            if upper:
                dsu[py, px] = piece
            else:
                dsg[px, py] = piece

    def both_parts(i, carry):
        dense_part(i, c, True)
        dense_part(i, c, False)
        return carry

    dense_rows(c)
    lax.fori_loop(0, 2, both_parts, 0)
    for d in Z_ORDER:
        p = lax.rem(z + NZ - d, NZ)
        wait_for(resall.at[p, 1 - c], z2sem.at[0, p])
    dense_rows(1 - c)
    lax.fori_loop(0, 2, lambda i, carry: (dense_part(i, 1 - c, True), carry)[1], 0)
    for d in (2, 1, 3):
        py = lax.rem(ey + d, 4)
        rcopy(dsu.at[py], r1u.at[ey], ssem.at[24], gsem.at[1], 4 * py + ex_, t).start()
    lax.fori_loop(0, 2, lambda i, carry: (dense_part(i, 1 - c, False), carry)[1], 0)

    def dense_stats(g, carry):
        rows = pl.ds(pl.multiple_of(g * 128, 128), 128)
        stat = dot_rows(jnp.ones((8, COLS), BF16), r2all[rows, :])
        br = dot_rows(jnp.broadcast_to(w_b, (8, COLS)), aall[rows, :])
        sub8 = lax.broadcasted_iota(jnp.int32, (8, 128), 0)
        stsend[g] = jnp.where(sub8 < 4, stat, br)
        return carry

    for d in (2, 1, 3):
        px = lax.rem(ex_ + d, 4)
        rcopy(dsg.at[px], r1g.at[ex_], ssem.at[11], gsem.at[0], 4 * ey + px, t).start()
    mark("m_wait_dispatch")
    wait_for(xsa.at[0:15], rsem.at[5])
    wait_for(xsb.at[0:15], rsem.at[15])

    def to_z(p):
        for ref, i, k in ((xfa, 10, 1), (xfb, 28, 3)):
            part_ = ref.at[z, :, half(c)]
            rcopy(part_, part_, ssem.at[i], zsem.at[k, z], e, 2 * p + c).start()

    over_z(to_z)
    lax.fori_loop(0, 4, dense_stats, 0)
    over_ep(lambda p: rcopy(stsend.at[p // 4], strecv.at[e], ssem.at[12], rsem.at[7], p, t).start())
    r1g[ex_] = dsg[ex_]
    r1u[ey] = dsu[ey]
    strecv[e] = stsend[e // 4]

    mark("o_expert_fwd")
    def second_stage():
        for parts, got, mine, left, sem in ((r1g, d2g, ey, r2g, 0), (r1u, d2u, ex_, r2u, 1)):
            wait_for(parts.at[0:3], gsem.at[sem])
            for k in range(4):
                tot = parts[0, k].astype(F32) + parts[1, k].astype(F32)
                got[k] = (tot + parts[2, k].astype(F32) + parts[3, k].astype(F32)).astype(BF16)
            left[mine] = got[mine]
            for d in (2, 1, 3):
                other = lax.rem(mine + d, 4)
                target = 4 * other + ex_ if sem == 0 else 4 * ey + other
                rcopy(got.at[other], left.at[mine], ssem.at[25 + sem], gsem.at[2 + sem], target, t).start()

    for d in Z_ORDER:
        p = lax.rem(z + NZ - d, NZ)
        for ref, i, k in ((xfa, 13, 1), (xfb, 29, 3)):
            part_ = ref.at[p, :, half(c)]
            wait_for(part_, zsem.at[k, p])
            rcopy(part_, part_, ssem.at[i], z2sem.at[k, p], e, mate).start()
        if d == Z_ORDER[SECOND_AT]:
            second_stage()

    mark("p_wait_dense")
    wait_for(r2g.at[0:3], gsem.at[2])
    wait_for(r2u.at[0:3], gsem.at[3])
    wait_for(strecv.at[0:15], rsem.at[7])
    mark("q_hidden")
    stats = strecv[0]
    for i in range(1, N):
        stats = stats + strecv[i]
    lane = lax.broadcasted_iota(jnp.int32, (ROWS, 128), 1)
    at = lane == lax.broadcasted_iota(jnp.int32, (ROWS, 128), 0) + ROWS * lax.rem(e, 4)
    sumsq = jnp.sum(jnp.where(at, stats[0:1, :], 0.0), axis=1, keepdims=True)
    branch = jnp.sum(jnp.where(at, stats[4:5, :], 0.0), axis=1, keepdims=True)
    rstd2 = lax.rsqrt(sumsq * (1.0 / D) + EPS)
    branch_share = jax.nn.sigmoid(branch * rstd2)
    hidden = [None, None]
    for h in range(2):
        cg = slice(256 * h, 256 * h + 256)
        g_ = r2g[0, :, cg].astype(F32)
        u_ = r2u[0, :, cg].astype(F32)
        for i in range(1, 4):
            g_ = g_ + r2g[i, :, cg].astype(F32)
            u_ = u_ + r2u[i, :, cg].astype(F32)
        g_ = g_ * rstd2
        u_ = u_ * rstd2
        hidden[h] = (g_ * jax.nn.sigmoid(g_) * u_ * branch_share).astype(BF16)
    halla[ey, ex_] = hidden[0]
    hallb[ex_, ey] = hidden[1]
    for d in (2, 1, 3):
        px, py = lax.rem(ex_ + d, 4), lax.rem(ey + d, 4)
        rcopy(halla.at[ey, ex_], halla.at[ey, ex_], ssem.at[14], lsem.at[0], 4 * ey + px, t).start()
        rcopy(hallb.at[ex_, ey], hallb.at[ex_, ey], ssem.at[30], lsem.at[1], 4 * py + ex_, t).start()

    mark("r_wait_expert")
    for i in (20, 21, 22):
        copies[i].wait()
    for d in Z_ORDER:
        p = lax.rem(z + NZ - d, NZ)
        wait_for(xfa.at[p, :, half(1 - c)], z2sem.at[1, p])
        wait_for(xfb.at[p, :, half(1 - c)], z2sem.at[3, p])

    mark("r2_rows")
    def expert_rows(k, carry):
        tot = jnp.zeros((16, 128), F32)

        def rows_of(cut):
            third = xfb[k, :, cut].astype(F32)
            return jnp.concatenate([xfa[k, :, cut].astype(F32), third, jnp.zeros_like(third)], axis=0)

        for m in range(4):
            wide = rows_of(slice(1024 * m, 1024 * m + 1024))
            sq = wide * wide
            for n in range(8):
                tot = tot + sq[:, 128 * n:128 * n + 128]
        scale = lax.rsqrt(jnp.sum(tot, axis=1, keepdims=True) * (1.0 / D) + EPS)
        rows = pl.ds(pl.multiple_of(k * 16, 16), 16)
        for m in range(4):
            cut = slice(1024 * m, 1024 * m + 1024)
            aexp[rows, cut] = (rows_of(cut) * scale * gffn[:, cut]).astype(BF16)
        return carry

    lax.fori_loop(0, NZ, expert_rows, 0)
    mark("s_expert")
    acc[...] = jnp.zeros_like(acc)

    def expert_in(k, carry):
        cut = pl.ds(pl.multiple_of(k * 512, 512), 512)
        lhs = aexp[:, cut]
        acc[:, 0:256] += dot(lhs, eg[cut, :])
        acc[:, 256:512] += dot(lhs, eu[cut, :])
        return carry

    lax.fori_loop(0, 8, expert_in, 0)
    g_ = acc[:, 0:256]
    hid = (g_ * jax.nn.sigmoid(g_) * acc[:, 256:512]).astype(BF16)
    aexp[:, 0:256] = hid

    mark("s3_hidden_stage")
    wait_for(halla.at[0, 0:3], lsem.at[0])
    wait_for(hallb.at[0, 0:3], lsem.at[1])
    for d in (2, 1, 3):
        px, py = lax.rem(ex_ + d, 4), lax.rem(ey + d, 4)
        rcopy(halla.at[ey], halla.at[ey], ssem.at[31], lsem.at[2], 4 * py + ex_, t).start()
        rcopy(hallb.at[ex_], hallb.at[ex_], ssem.at[32], lsem.at[3], 4 * ey + px, t).start()
    mark("s2_expert_out")

    def chunk_of(k):
        return lax.rem(k + e, 4)

    def expert_out(part_, k):
        at_ = pl.ds(pl.multiple_of(part_ * HALF + k * 512, 512), 512)
        return dot(aexp[:, 0:256], ed[:, at_])

    def for_mate(i, carry):
        k = chunk_of(i)
        prod = expert_out(1 - c, k).astype(BF16)
        for n in range(NZ):
            yp[k, n] = prod[16 * n:16 * n + 16]
        rcopy(yp.at[k], yd2d.at[k], ssem.at[15], dsem.at[k], e, mate).start()
        return carry

    def back(j, pe):
        rcopy(ys.at[1 - c, :, :, cols(j)], yin.at[:, e], ssem.at[18], rsem.at[12], pe, mate).start()

        @pl.when(pe != e)
        def _():
            rcopy(ys.at[c, :, :, cols(j)], yin.at[:, e], ssem.at[19], rsem.at[12], pe, t).start()

        @pl.when(pe == e)
        def _():
            yin[:, e] = ys[c, :, :, cols(j)]

    def for_own(i, carry):
        k = chunk_of(i)
        prod = expert_out(c, k)
        at_ = pl.ds(pl.multiple_of(k * 512, 512), 512)
        wait_for(yd2d.at[k], dsem.at[k])
        both_sum = jnp.concatenate([prod[16 * n:16 * n + 16] + yd2d[k, n].astype(F32) for n in range(NZ)], axis=0)
        compact = dot(keep_rows, both_sum.astype(BF16))
        for n in range(4):
            ys[n // 2, n % 2, :, at_] = compact[24 * n:24 * n + 24].astype(BF16)
        for j in range(2):
            back(2 * k + j, c * NZ + 2 * k + j)
        return carry

    lax.fori_loop(0, 4, for_mate, 0)
    lax.fori_loop(0, 4, for_own, 0)

    mark("t_wait_hidden")
    copies[19].wait()
    wait_for(halla.at[0:3], lsem.at[2])
    wait_for(hallb.at[0:3], lsem.at[3])
    mark("u_down")

    def dense_down(g, carry):
        left = jnp.concatenate([halla[g, j] for j in range(4)], axis=0)
        right = jnp.concatenate([hallb[j, g] for j in range(4)], axis=0)
        prod = dot(jnp.concatenate([left, right], axis=1), dd[...])
        for j in range(4):
            part2[2 * g + j // 2, j % 2] = prod[32 * j:32 * j + 32].astype(BF16)
        return carry

    lax.fori_loop(0, 4, dense_down, 0)
    rcopy(part2.at[:, 1 - c], pd2d2, ssem.at[16], rsem.at[10], e, mate).start()
    mark("v_wait_back")
    either(e // NZ == c, yin.at[:, 0:15], yin, rsem.at[12])
    wait_for(pd2d2, rsem.at[10])
    mark("w_combine")

    for g in range(2):
        rows = yin[g].astype(F32).reshape(384, COLS).astype(BF16)
        tot = dot(wtab[g, 0], rows) + dot(wtab[g, 1], rows)
        for m in range(4):
            k = 4 * g + m
            total_ = tot[32 * m:32 * m + 32] + part2[k, c].astype(F32) + pd2d2[k].astype(F32)
            rsend2[k] = total_.astype(BF16)
    over_z(lambda p: rcopy(rsend2.at[p], rrecv2.at[z], ssem.at[17], rsem.at[11], e, 2 * p + c).start())
    rrecv2[z] = rsend2[z]
    mark("x_wait_rs")
    wait_for(rrecv2.at[0:7], rsem.at[11])
    tot = resall[z, c].astype(F32)
    for k in range(NZ):
        tot = tot + rrecv2[k].astype(F32)
    outv[...] = tot.astype(BF16)

    mark("z_deliver")
    def deliver(d):
        p = lax.rem(z + d, NZ)

        @pl.when(jnp.logical_or(t != e, p != z))
        def _():
            rcopy(outv, ofull.at[:, cols(e)], ssem.at[20], osem.at[e], t, 2 * p + c).start()

    for d in Z_ORDER + (0,):
        deliver(d)

    @pl.when(t == e)
    def _():
        ofull[:, cols(e)] = outv[...]

    first = c == lax.rem(e, 2)

    @pl.when(first)
    def _():
        def pass_on(d, carry):
            p = down(d)

            @pl.when(jnp.logical_or(t != e, p != e))
            def _():
                wait_for(ofull.at[:, cols(p)], osem.at[p])

            rcopy(ofull.at[:, cols(p)], ofull.at[:, cols(p)], ssem.at[22], rsem.at[14], e, mate).start()
            return carry

        lax.fori_loop(0, N, pass_on, 0)
        wait_for(ofull, ssem.at[22])

    @pl.when(jnp.logical_not(first))
    def _():
        wait_for(ofull, rsem.at[14])

    mark("zz_end")
    wait_for(xall.at[0:15], ssem.at[0])
    wait_for(rtall.at[0:15], ssem.at[1])
    wait_for(csend.at[0:15], ssem.at[2])
    wait_for(heads.at[:, 0:15 * HD], ssem.at[3])
    wait_for(mhall.at[0:15], ssem.at[23])
    wait_for(wp, ssem.at[4])
    wait_for(wpall.at[0:7 * HD], ssem.at[5])
    wait_for(resall.at[0, 0], ssem.at[6])
    wait_for(rsend2.at[0:7], ssem.at[7])
    wait_for(xsa.at[0:15], ssem.at[8])
    wait_for(xsb.at[0:15], ssem.at[27])
    wait_for(rsend2.at[0:7], ssem.at[9])
    wait_for(xfa.at[0:7, :, 0:HALF], ssem.at[10])
    wait_for(xfb.at[0:7, :, 0:HALF], ssem.at[28])
    for i, ref in ((11, dsg), (24, dsu), (25, d2g), (26, d2u)):
        wait_for(ref.at[0:3], ssem.at[i])
    wait_for(strecv.at[0:15], ssem.at[12])
    wait_for(xfa.at[0:7, :, 0:HALF], ssem.at[13])
    wait_for(xfb.at[0:7, :, 0:HALF], ssem.at[29])
    for i, ref in ((14, halla.at[0]), (30, hallb.at[0]), (31, halla), (32, hallb)):
        wait_for(ref.at[0:3], ssem.at[i])
    wait_for(yd2d, ssem.at[15])
    wait_for(pd2d2, ssem.at[16])
    wait_for(rsend2.at[0:7], ssem.at[17])
    wait_for(yin.at[:, 0:8], ssem.at[18])
    either(e // NZ == c, yin.at[:, 0:7], yin.at[:, 0:8], ssem.at[19])
    either(t == e, rsend2.at[0:7], rsend2, ssem.at[20])
    wait_for(wpall.at[0:7 * HD], ssem.at[21])
    mark(None)


def finish_kernel(out_v, nm_v, nn_v, nmax_v, out_o, nm_o, nn_o, nmax_o, sem):
    trips = [(nm_v.at[8 * k:8 * k + 8], nm_o.at[8 * k:8 * k + 8]) for k in range(4)]
    trips += [(out_v, out_o), (nn_v, nn_o), (nmax_v, nmax_o)]
    copies = [pltpu.make_async_copy(a, b, sem.at[i]) for i, (a, b) in enumerate(trips)]
    for copy in copies:
        copy.start()
    for copy in copies:
        copy.wait()


def on_device(
    tokens, state_matrix, state_norm, state_max, mixer_gain, w_query, w_key, w_value, w_outgate, w_ingate, w_forget,
    forget_bias, w_proj, ffn_gain, w_branch, routes, route_weight, expert_gate, expert_up, expert_down,
    dense_gate, dense_up, dense_down,
):
    any_ = pl.BlockSpec(memory_space=pltpu.HBM)
    local = pl.BlockSpec(memory_space=pltpu.VMEM)
    vm = pltpu.VMEM
    scratch = [
        vm((ROWS, D), BF16), vm((ROWS, HD, HD), F32), vm((ROWS, HD), F32), vm((1, ROWS), F32), vm((1, D), F32),
        vm((COLS, 512), BF16), vm((N, D), BF16), vm((N, D), BF16), vm((1, N), F32), vm((HD, COLS), BF16),
        vm((1, D), F32), vm((ROWS, HD), BF16), vm((2, ROWS), jnp.int32), vm((2, ROWS), F32),
        vm((D, COLS), BF16), vm((D, COLS), BF16), vm((COLS, D), BF16), vm((COLS, 1024), BF16), vm((512, COLS), BF16),
        vm((N, ROWS, COLS), BF16), vm((N, ROWS, 512), BF16), vm((N, ROWS, 512), BF16), vm((N, ROWS, HD), BF16),
        vm((ROWS, HALF), BF16), vm((ROWS, HD), F32),
        vm((HALF, COLS), BF16), vm((2, 2, 128, 384), BF16), vm((NZ, 2, ROWS, COLS), BF16),
        vm((NZ, 2, ROWS, COLS), BF16), vm((NZ, ROWS, COLS), BF16), vm((NZ, ROWS, COLS), BF16),
        vm((NZ, ROWS, COLS), BF16),
        vm((8, 128), F32), vm((N, 8, 128), F32),
        vm((4, 4, ROWS, 512), BF16), vm((4, 4, ROWS, 512), BF16), vm((4, 4, ROWS, 512), BF16),
        vm((4, 4, ROWS, 512), BF16), vm((4, ROWS, 512), BF16), vm((4, ROWS, 512), BF16), vm((4, ROWS, 512), BF16),
        vm((4, ROWS, 512), BF16),
        vm((4, 8, 128), F32), vm((N, 8, 128), F32), vm((4, 4, ROWS, COLS), BF16),
        vm((4, 4, ROWS, COLS), BF16), vm((512, COLS), BF16),
        vm((512, COLS), BF16),
        vm((N, 8, COLS), BF16), vm((N, 4, COLS), BF16), vm((NZ, 8, D), BF16), vm((NZ, 4, D), BF16), vm((128, D), BF16), vm((128, 512), F32),
        vm((4, NZ, 16, 512), BF16), vm((4, NZ, 16, 512), BF16), vm((2, 2, 24, HALF), BF16), vm((2, N, 24, COLS), BF16),
        vm((ROWS, COLS), BF16),
        pltpu.SemaphoreType.DMA((23,)), pltpu.SemaphoreType.DMA((33,)), pltpu.SemaphoreType.DMA((N,)),
        pltpu.SemaphoreType.DMA((16,)), pltpu.SemaphoreType.DMA((4, NZ)), pltpu.SemaphoreType.DMA((4, NZ)),
        pltpu.SemaphoreType.DMA((N,)), pltpu.SemaphoreType.DMA((N,)), pltpu.SemaphoreType.DMA((4,)),
        pltpu.SemaphoreType.DMA((4,)), pltpu.SemaphoreType.DMA((4,)),
    ]
    results = pl.pallas_call(
        layer_kernel,
        out_shape=(vm((ROWS, D), BF16), vm((ROWS, HD, HD), F32), vm((ROWS, HD), F32), vm((1, ROWS), F32)),
        in_specs=[any_] * 23,
        out_specs=(local,) * 4,
        scratch_shapes=scratch,
        compiler_params=pltpu.CompilerParams(
            collective_id=0, has_side_effects=True, vmem_limit_bytes=60 * 1024 * 1024
        ),
        name="layer",
    )(
        tokens, state_matrix.reshape(ROWS, HD, HD), state_norm.reshape(ROWS, HD), state_max.T,
        mixer_gain.reshape(1, D), w_query, w_key, w_value, w_outgate, w_ingate.T, w_forget.T,
        forget_bias.reshape(1, N), w_proj, ffn_gain.reshape(1, D), w_branch.reshape(ROWS, HD), routes.T,
        route_weight.T, expert_gate, expert_up, expert_down, dense_gate, dense_up, dense_down,
    )
    out, nm, nn, nmax = pl.pallas_call(
        finish_kernel,
        out_shape=(
            jax.ShapeDtypeStruct((ROWS, D), BF16), jax.ShapeDtypeStruct((ROWS, HD, HD), F32),
            jax.ShapeDtypeStruct((ROWS, HD), F32), jax.ShapeDtypeStruct((1, ROWS), F32),
        ),
        in_specs=[local] * 4,
        out_specs=(any_,) * 4,
        scratch_shapes=[pltpu.SemaphoreType.DMA((7,))],
        compiler_params=pltpu.CompilerParams(vmem_limit_bytes=8 * 1024 * 1024),
        name="finish",
    )(*results)
    return (
        out, nm.reshape(ROWS, 1, HD, HD), nn.reshape(ROWS, 1, HD), nmax.T,
    )


def solution(mesh):
    in_specs = (
        P("ep", None), P("ep", "tp", None, None), P("ep", "tp", None), P("ep", "tp"), P(),
        P("ep", "tp"), P("ep", "tp"), P("ep", "tp"), P("ep", "tp"), P(), P(), P(), P("tp", "ep"), P(), P(),
        P("ep", None), P("ep", None), P("ep", None, "tp"), P("ep", None, "tp"), P("ep", "tp", None),
        P("ep", "tp"), P("ep", "tp"), P("tp", "ep"),
    )
    out_specs = (P("ep", None), P("ep", "tp", None, None), P("ep", "tp", None), P("ep", "tp"))
    return jax.shard_map(on_device, mesh=mesh, in_specs=in_specs, out_specs=out_specs, check_vma=False)
```

```python
import functools

import jax
import jax.numpy as jnp
from jax import lax
from jax.experimental import pallas as pl
from jax.experimental.pallas import tpu as pltpu
from jax.sharding import PartitionSpec as P

EPS = 1e-06
MESH = pl.DeviceIdType.MESH
F32 = jnp.float32
BF16 = jnp.bfloat16
N = 16
NZ = 8
ROWS = 32
D = 4096
COLS = 256
HALF = 2048
HD = 128
SECOND_AT = 0
HOPS = (0, 1, 2, 1)
EP_ORDER = sorted(
    [(dy, dx) for dy in range(4) for dx in range(4) if dy + dx], key=lambda o: -(HOPS[o[0]] + HOPS[o[1]])
)
Z_ORDER = (4, 3, 5, 2, 6, 1, 7)


def dot(a, b):
    return jnp.dot(a, b, preferred_element_type=F32)


def dot_rows(a, b):
    return lax.dot_general(a, b, (((1,), (1,)), ((), ())), preferred_element_type=F32)


def layer_kernel(
    tok_h, st_h, sn_h, smax_h, gmix_h, wq_h, wk_h, wv_h, wo_h, wi_h, wf_h, fb_h, wp_h, gffn_h, wbr_h,
    rt_h, rw_h, eg_h, eu_h, ed_h, dg_h, du_h, dd_h,
    ofull, nm, nnv, nmaxv,
    tok, st, sn, smax, gmix, wq, wi, wf, fb, wp, gffn, wbr, rt, rw, eg, eu, ed, dgu, dd,
    xall, csend, crecv, mhall, heads, num,
    wpall, wtab, resall,
    part2, pd2d2, rsend2, rrecv2,
    rtsend, rtall, dsg, dsu, r1g, r1u, d2g, d2u, r2g, r2u, stsend, strecv, halla, hallb, hallc, r2all, aall,
    xsa, xsb, xfa, xfb, aexp, acc, yp, yd2d, ys, yin, outv,
    load_sem, ssem, bsem, rsem, zsem, z2sem, osem, hsem, gsem, dsem, lsem,
):
    e = lax.axis_index("ep")
    t = lax.axis_index("tp")
    z = t // 2
    c = lax.rem(t, 2)
    mate = 2 * z + 1 - c
    ey, ex_ = e // 4, lax.rem(e, 4)

    def rcopy(src, dst, send, recv, pe, pt):
        return pltpu.make_async_remote_copy(
            src_ref=src, dst_ref=dst, send_sem=send, recv_sem=recv, device_id=(pe, pt), device_id_type=MESH
        )

    def wait_for(ref, sem):
        pltpu.make_async_copy(ref, ref, sem).wait()

    def either(less, ref_less, ref_all, sem):
        @pl.when(less)
        def _():
            wait_for(ref_less, sem)

        @pl.when(jnp.logical_not(less))
        def _():
            wait_for(ref_all, sem)

    def ahead(offset):
        return 4 * lax.rem(ey + offset[0], 4) + lax.rem(ex_ + offset[1], 4)

    def behind(offset):
        return 4 * lax.rem(ey + 4 - offset[0], 4) + lax.rem(ex_ + 4 - offset[1], 4)

    def down(d):
        return lax.rem(e + N - d, N)

    def over_ep(fn):
        for offset in EP_ORDER:
            fn(ahead(offset))

    def over_z(fn):
        for d in Z_ORDER:
            fn(lax.rem(z + d, NZ))

    def cols(index):
        return pl.ds(pl.multiple_of(index * COLS, COLS), COLS)

    def half(index):
        return pl.ds(pl.multiple_of(index * HALF, HALF), HALF)

    scopes = []

    def mark(name):
        if scopes:
            scopes.pop().__exit__(None, None, None)
        if name:
            scopes.append(jax.named_scope(name))
            scopes[-1].__enter__()

    mark("a_barrier")
    loads = [
        (tok_h, tok), (gmix_h, gmix),
        (wq_h, wq.at[:, 0:128]), (wk_h, wq.at[:, 128:256]), (wv_h, wq.at[:, 256:384]), (wo_h, wq.at[:, 384:512]),
        (wi_h, wi), (wf_h, wf), (fb_h, fb), (smax_h, smax), (sn_h, sn), (st_h, st), (wp_h, wp), (gffn_h, gffn),
        (wbr_h, wbr), (rt_h, rt), (rw_h, rw), (dg_h, dgu.at[:, 0:512]), (du_h, dgu.at[:, 512:1024]), (dd_h, dd),
        (eg_h.at[0], eg), (eu_h.at[0], eu), (ed_h.at[0], ed),
    ]
    copies = [pltpu.make_async_copy(s, d, load_sem.at[i]) for i, (s, d) in enumerate(loads)]
    for copy in copies:
        copy.start()

    barrier = pltpu.get_barrier_semaphore()

    def greet_ep(p):
        pl.semaphore_signal(barrier, inc=1, device_id=(p, t), device_id_type=MESH)

    def greet_tp(d, carry):
        pl.semaphore_signal(barrier, inc=1, device_id=(e, lax.rem(t + d, N)), device_id_type=MESH)
        return carry

    over_ep(greet_ep)
    lax.fori_loop(1, N, greet_tp, 0)
    copies[0].wait()
    copies[1].wait()
    pl.semaphore_wait(barrier, 2 * (N - 1))

    mark("b_spread_gates")
    over_ep(lambda p: rcopy(tok.at[:, cols(p)], xall.at[e], ssem.at[0], bsem.at[e], p, t).start())
    copies[12].wait()
    mine_wp = wpall.at[pl.ds(pl.multiple_of(t * HD, HD), HD), :]
    rcopy(wp, mine_wp, ssem.at[4], z2sem.at[2, z], e, mate).start()
    over_z(lambda p: rcopy(wp, mine_wp, ssem.at[5], zsem.at[2, z], e, 2 * p + c).start())
    wpall[pl.ds(pl.multiple_of(t * HD, HD), HD), :] = wp[...]
    xall[e] = tok[:, cols(e)]
    gain_e = gmix[:, cols(e)]

    total = jnp.zeros((ROWS, 128), F32)
    for k in range(8):
        wide = tok[:, k * 512:(k + 1) * 512].astype(F32)
        sq = wide * wide
        total = total + (sq[:, 0:128] + sq[:, 128:256]) + (sq[:, 256:384] + sq[:, 384:512])
    rstd = lax.rsqrt(jnp.sum(total, axis=1, keepdims=True) * (1.0 / D) + EPS)
    for i in (6, 7, 8, 9, 15, 16):
        copies[i].wait()
    gi = jnp.zeros((ROWS, N), F32)
    gf = jnp.zeros((ROWS, N), F32)
    for k in range(8):
        cut = slice(k * 512, (k + 1) * 512)
        nb = (tok[:, cut].astype(F32) * rstd * gmix[:, cut]).astype(BF16)
        gi = gi + dot_rows(nb, wi[:, cut])
        gf = gf + dot_rows(nb, wf[:, cut])
    gf = gf + fb[...]
    mine = lax.broadcasted_iota(jnp.int32, (ROWS, N), 1) == t
    gate_in = jnp.sum(jnp.where(mine, gi, 0.0), axis=1, keepdims=True)
    gate_f = jnp.sum(jnp.where(mine, gf, 0.0), axis=1, keepdims=True)
    log_keep = jnp.minimum(gate_f, 0.0) - jnp.log1p(jnp.exp(-jnp.abs(gate_f)))
    square = lax.broadcasted_iota(jnp.int32, (ROWS, ROWS), 0) == lax.broadcasted_iota(jnp.int32, (ROWS, ROWS), 1)
    kept = log_keep + jnp.sum(jnp.where(square, smax[...], 0.0), axis=1, keepdims=True)
    new_max = jnp.maximum(kept, gate_in)
    keep = jnp.exp(kept - new_max)
    write = jnp.exp(gate_in - new_max)
    nmaxv[...] = jnp.sum(jnp.where(square, new_max, 0.0), axis=0, keepdims=True)
    rtsend[...] = jnp.full((8, 128), -1.0, F32)
    rtsend[0:2, 0:ROWS] = rt[...].astype(F32)
    rtsend[2:4, 0:ROWS] = rw[...]
    over_ep(lambda p: rcopy(rtsend, rtall.at[e], ssem.at[1], rsem.at[0], p, t).start())
    rtall[e] = rtsend[...]
    for i in (2, 3, 4, 5, 10, 11):
        copies[i].wait()

    mark("c_qkvo_part")
    for g in range(4):
        ps = [e if 4 * g + j == 0 else behind(EP_ORDER[4 * g + j - 1]) for j in range(4)]
        for j in range(4):
            if 4 * g + j:
                wait_for(xall.at[ps[j]], bsem.at[ps[j]])
        block = jnp.concatenate([xall[p] for p in ps], axis=0)
        prod = dot((block.astype(F32) * gain_e).astype(BF16), wq[...])
        for j in range(4):
            piece = prod[32 * j:32 * j + 32].astype(BF16)
            if 4 * g + j:
                csend[ps[j]] = piece
                rcopy(csend.at[ps[j]], crecv.at[e], ssem.at[2], rsem.at[1], ps[j], t).start()
            else:
                crecv[e] = piece
    mark("d_wait_qkvo")
    keep_w = jnp.broadcast_to(keep, (ROWS, HD))
    for b in range(ROWS):
        st[b] = keep_w[b:b + 1, :] * st[b]
    wait_for(crecv.at[0:15], rsem.at[1])
    mark("e_cell")
    qkvo = crecv[0].astype(F32)
    for i in range(1, N):
        qkvo = qkvo + crecv[i].astype(F32)
    qkvo = qkvo * rstd
    q = qkvo[:, 0:128]
    kw = qkvo[:, 128:256] * (HD ** -0.5) * write
    v = qkvo[:, 256:384]
    new_norm = keep_w * sn[...] + kw
    nnv[...] = new_norm
    q_t = jnp.transpose(q)
    for b in range(ROWS):
        num[b:b + 1, :] = jnp.sum(q_t[:, b:b + 1] * st[b], axis=0, keepdims=True)
    numer = num[...] + jnp.sum(q * kw, axis=1, keepdims=True) * v
    denom = jnp.maximum(jnp.abs(jnp.sum(q * new_norm, axis=1, keepdims=True)), 1.0)
    mhall[e] = (jax.nn.sigmoid(qkvo[:, 384:512]) * (numer / denom)).astype(BF16)
    over_ep(lambda p: rcopy(mhall.at[e], mhall.at[e], ssem.at[23], hsem.at[e], p, t).start())
    kw_t = jnp.transpose(kw)
    for b in range(ROWS):
        nm[b] = st[b] + kw_t[:, b:b + 1] * v[b:b + 1, :]
    head_cols = pl.ds(pl.multiple_of(t * HD, HD), HD)

    def turn_heads(p):
        @pl.when(p != t)
        def _():
            rcopy(mhall.at[p], heads.at[:, head_cols], ssem.at[3], rsem.at[2], e, p).start()

        @pl.when(p == t)
        def _():
            heads[:, head_cols] = mhall[p]

    mark("f_tables")
    wait_for(rtall.at[0:15], rsem.at[0])
    before = (lax.broadcasted_iota(jnp.int32, (128, 128), 0) < lax.broadcasted_iota(jnp.int32, (128, 128), 1)).astype(BF16)
    row8 = lax.broadcasted_iota(jnp.int32, (128, 128), 0)
    row_e = (row8 // 8).astype(F32)
    row16 = lax.broadcasted_iota(jnp.int32, (256, 128), 0)
    row16_e = (row16 // 16).astype(F32)
    row16_q = lax.rem(row16, 16)

    def pick_table(group, low):
        info = rtall[group]
        hit = jnp.logical_or(info[0:1, :] == row16_e, info[1:2, :] == row16_e).astype(F32)
        slot = dot(hit.astype(BF16), before)
        inside = jnp.logical_and(row16_q >= low, row16_q < low + 6)
        fits = jnp.logical_and(slot == (row16_q - low).astype(F32), inside).astype(F32)
        return (hit * fits)[:, 0:ROWS].astype(BF16)

    row_s = lax.rem(row8, 8).astype(F32)

    def table(group):
        info = rtall[group]
        first = (info[0:1, :] == row_e).astype(F32)
        second = (info[1:2, :] == row_e).astype(F32)
        slot = dot((first + second).astype(BF16), before)
        fits = (slot == row_s).astype(F32)
        share = 1.0 / (info[2:3, :] + info[3:4, :])
        weigh = (first * (info[2:3, :] * share) + second * (info[3:4, :] * share)) * fits
        return weigh

    pick0 = pick_table(2 * z, 0)
    pick1 = pick_table(2 * z + 1, 6)

    def wp_rows(index):
        return wpall.at[pl.ds(pl.multiple_of(index * HD, HD), HD), :]

    for d in Z_ORDER:
        p = lax.rem(z + NZ - d, NZ)
        wait_for(wp_rows(2 * p + c), zsem.at[2, p])
        rcopy(wp_rows(2 * p + c), wp_rows(2 * p + c), ssem.at[21], z2sem.at[2, p], e, mate).start()
    for d in Z_ORDER + (0,):
        for k in range(2):
            p = 2 * lax.rem(z + d, NZ) + k

            @pl.when(p != e)
            def _(p=p):
                wait_for(mhall.at[p], hsem.at[p])

            turn_heads(p)
    mark("g_wait_heads")
    def combine_table(k, carry):
        turned = jnp.transpose(table(2 * k + c))[0:ROWS, :]
        high = turned.astype(BF16)
        low = (turned - high.astype(F32)).astype(BF16)
        m = lax.rem(k, 4)
        r = lax.broadcasted_iota(jnp.int32, (128, 384), 0)
        q = lax.broadcasted_iota(jnp.int32, (128, 384), 1)
        same = jnp.logical_and(r // 8 == q // 24, lax.rem(q, 24) == 6 * m + lax.rem(r, 8))
        move = jnp.logical_and(same, lax.rem(r, 8) < 6).astype(F32).astype(BF16)
        moved = dot(jnp.concatenate([high, low], axis=0), move).astype(BF16)
        rows = pl.ds(pl.multiple_of(m * ROWS, ROWS), ROWS)
        wtab[k // 4, 0, rows, :] = moved[0:ROWS]
        wtab[k // 4, 1, rows, :] = moved[ROWS:2 * ROWS]
        return carry

    lax.fori_loop(0, NZ, combine_table, 0)
    rr = lax.broadcasted_iota(jnp.int32, (96, 128), 0)
    rq = lax.broadcasted_iota(jnp.int32, (96, 128), 1)
    rest = lax.rem(rr, 48)
    keep_rows = (rq == 16 * (rest // 6) + lax.rem(rest, 6) + 6 * (rr // 48)).astype(F32).astype(BF16)

    for d in range(NZ):
        p = lax.rem(z + NZ - d, NZ)
        wait_for(wp_rows(2 * p + 1 - c), z2sem.at[2, p])

    wait_for(heads.at[:, 0:15 * HD], rsem.at[2])
    mark("h_proj")
    mix = dot(heads[...], wpall[...])
    res_own = (xall[t].astype(F32) + mix).astype(BF16)
    resall[z, c] = res_own

    mark("j_ag_send")
    rcopy(resall.at[z, c], resall.at[z, c], ssem.at[6], z2sem.at[0, z], e, mate).start()
    over_z(lambda p: rcopy(resall.at[z, c], resall.at[z, c], ssem.at[7], zsem.at[0, z], e, 2 * p + c).start())
    mark("k_wait_mate_dispatch")
    wait_for(resall.at[z, 1 - c], z2sem.at[0, z])
    routed = dot(pick0, resall[z, 0]) + dot(pick1, resall[z, 1])
    for ex in range(N):
        xsa[ex] = routed[16 * ex:16 * ex + 8].astype(BF16)
        xsb[ex] = routed[16 * ex + 8:16 * ex + 12].astype(BF16)
    over_ep(lambda p: rcopy(xsa.at[p], xfa.at[z, :, cols(e)], ssem.at[8], rsem.at[5], p, t).start())
    over_ep(lambda p: rcopy(xsb.at[p], xfb.at[z, :, cols(e)], ssem.at[27], rsem.at[15], p, t).start())
    xfa[z, :, cols(e)] = xsa[e]
    xfb[z, :, cols(e)] = xsb[e]

    for i in (13, 14, 17, 18):
        copies[i].wait()
    mark("l_ag_forward")
    gain_f = gffn[:, cols(e)]
    sub = lax.broadcasted_iota(jnp.int32, (ROWS, HD), 0)
    w_rows = wbr[...].astype(F32)
    w_b = jnp.concatenate(
        [jnp.sum(jnp.where(sub == 2 * e + k, w_rows, 0.0), axis=0, keepdims=True) for k in range(2)], axis=1
    ).astype(BF16)

    for d in Z_ORDER:
        p = lax.rem(z + NZ - d, NZ)
        wait_for(resall.at[p, c], zsem.at[0, p])
        rcopy(resall.at[p, c], resall.at[p, c], ssem.at[9], z2sem.at[0, p], e, mate).start()

    mark("n_wait_fwd_dense")
    def rows_for(k, par):
        return pl.ds(pl.multiple_of(64 * k + 32 * par, 32), 32)

    def dense_rows(par):
        for k in range(NZ):
            wide = resall[k, par].astype(F32)
            r2all[rows_for(k, par), :] = (wide * wide).astype(BF16)
            aall[rows_for(k, par), :] = (wide * gain_f).astype(BF16)

    def dense_part(i, par, upper):
        lhs = jnp.concatenate([aall[rows_for(4 * i + j, par), :] for j in range(4)], axis=0)
        prod = dot(lhs, dgu[:, 512:1024] if upper else dgu[:, 0:512])
        for j in range(4):
            piece = prod[32 * j:32 * j + 32].astype(BF16)
            py, px = 2 * i + j // 2, 2 * (j % 2) + par
            if upper:
                dsu[py, px] = piece
            else:
                dsg[px, py] = piece

    def both_parts(i, carry):
        dense_part(i, c, True)
        dense_part(i, c, False)
        return carry

    dense_rows(c)
    lax.fori_loop(0, 2, both_parts, 0)
    for d in Z_ORDER:
        p = lax.rem(z + NZ - d, NZ)
        wait_for(resall.at[p, 1 - c], z2sem.at[0, p])
    dense_rows(1 - c)
    lax.fori_loop(0, 2, lambda i, carry: (dense_part(i, 1 - c, True), carry)[1], 0)
    for d in (2, 1, 3):
        py = lax.rem(ey + d, 4)
        rcopy(dsu.at[py], r1u.at[ey], ssem.at[24], gsem.at[1], 4 * py + ex_, t).start()
    lax.fori_loop(0, 2, lambda i, carry: (dense_part(i, 1 - c, False), carry)[1], 0)

    def dense_stats(g, carry):
        rows = pl.ds(pl.multiple_of(g * 128, 128), 128)
        stat = dot_rows(jnp.ones((8, COLS), BF16), r2all[rows, :])
        br = dot_rows(jnp.broadcast_to(w_b, (8, COLS)), aall[rows, :])
        sub8 = lax.broadcasted_iota(jnp.int32, (8, 128), 0)
        stsend[g] = jnp.where(sub8 < 4, stat, br)
        return carry

    for d in (2, 1, 3):
        px = lax.rem(ex_ + d, 4)
        rcopy(dsg.at[px], r1g.at[ex_], ssem.at[11], gsem.at[0], 4 * ey + px, t).start()
    mark("m_wait_dispatch")
    wait_for(xsa.at[0:15], rsem.at[5])
    wait_for(xsb.at[0:15], rsem.at[15])

    def to_z(p):
        for ref, i, k in ((xfa, 10, 1), (xfb, 28, 3)):
            part_ = ref.at[z, :, half(c)]
            rcopy(part_, part_, ssem.at[i], zsem.at[k, z], e, 2 * p + c).start()

    over_z(to_z)
    lax.fori_loop(0, 4, dense_stats, 0)
    over_ep(lambda p: rcopy(stsend.at[p // 4], strecv.at[e], ssem.at[12], rsem.at[7], p, t).start())
    r1g[ex_] = dsg[ex_]
    r1u[ey] = dsu[ey]
    strecv[e] = stsend[e // 4]

    mark("o_expert_fwd")
    def second_stage():
        for parts, got, mine, left, sem in ((r1g, d2g, ey, r2g, 0), (r1u, d2u, ex_, r2u, 1)):
            wait_for(parts.at[0:3], gsem.at[sem])
            for k in range(4):
                tot = parts[0, k].astype(F32) + parts[1, k].astype(F32)
                got[k] = (tot + parts[2, k].astype(F32) + parts[3, k].astype(F32)).astype(BF16)
            left[mine] = got[mine]
            for d in (2, 1, 3):
                other = lax.rem(mine + d, 4)
                target = 4 * other + ex_ if sem == 0 else 4 * ey + other
                rcopy(got.at[other], left.at[mine], ssem.at[25 + sem], gsem.at[2 + sem], target, t).start()

    for d in Z_ORDER:
        p = lax.rem(z + NZ - d, NZ)
        for ref, i, k in ((xfa, 13, 1), (xfb, 29, 3)):
            part_ = ref.at[p, :, half(c)]
            wait_for(part_, zsem.at[k, p])
            rcopy(part_, part_, ssem.at[i], z2sem.at[k, p], e, mate).start()
        if d == Z_ORDER[SECOND_AT]:
            second_stage()

    mark("p_wait_dense")
    wait_for(r2g.at[0:3], gsem.at[2])
    wait_for(r2u.at[0:3], gsem.at[3])
    wait_for(strecv.at[0:15], rsem.at[7])
    mark("q_hidden")
    stats = strecv[0]
    for i in range(1, N):
        stats = stats + strecv[i]
    lane = lax.broadcasted_iota(jnp.int32, (ROWS, 128), 1)
    at = lane == lax.broadcasted_iota(jnp.int32, (ROWS, 128), 0) + ROWS * lax.rem(e, 4)
    sumsq = jnp.sum(jnp.where(at, stats[0:1, :], 0.0), axis=1, keepdims=True)
    branch = jnp.sum(jnp.where(at, stats[4:5, :], 0.0), axis=1, keepdims=True)
    rstd2 = lax.rsqrt(sumsq * (1.0 / D) + EPS)
    branch_share = jax.nn.sigmoid(branch * rstd2)
    hidden = [None, None]
    for h in range(2):
        cg = slice(256 * h, 256 * h + 256)
        g_ = r2g[0, :, cg].astype(F32)
        u_ = r2u[0, :, cg].astype(F32)
        for i in range(1, 4):
            g_ = g_ + r2g[i, :, cg].astype(F32)
            u_ = u_ + r2u[i, :, cg].astype(F32)
        g_ = g_ * rstd2
        u_ = u_ * rstd2
        hidden[h] = (g_ * jax.nn.sigmoid(g_) * u_ * branch_share).astype(BF16)
    halla[ey, ex_] = hidden[1][:, 0:128]
    hallb[ex_, ey] = hidden[1][:, 128:256]
    hallc[e] = hidden[0]
    for d in (2, 1, 3):
        px, py = lax.rem(ex_ + d, 4), lax.rem(ey + d, 4)
        rcopy(halla.at[ey, ex_], halla.at[ey, ex_], ssem.at[14], lsem.at[0], 4 * ey + px, t).start()
        rcopy(hallb.at[ex_, ey], hallb.at[ex_, ey], ssem.at[30], lsem.at[1], 4 * py + ex_, t).start()
    over_ep(lambda p: rcopy(hallc.at[e], hallc.at[e], ssem.at[33], rsem.at[8], p, t).start())

    mark("r_wait_expert")
    for i in (20, 21, 22):
        copies[i].wait()
    for d in Z_ORDER:
        p = lax.rem(z + NZ - d, NZ)
        wait_for(xfa.at[p, :, half(1 - c)], z2sem.at[1, p])
        wait_for(xfb.at[p, :, half(1 - c)], z2sem.at[3, p])

    mark("r2_rows")
    def expert_rows(k, carry):
        tot = jnp.zeros((16, 128), F32)

        def rows_of(cut):
            third = xfb[k, :, cut].astype(F32)
            return jnp.concatenate([xfa[k, :, cut].astype(F32), third, jnp.zeros_like(third)], axis=0)

        for m in range(4):
            wide = rows_of(slice(1024 * m, 1024 * m + 1024))
            sq = wide * wide
            for n in range(8):
                tot = tot + sq[:, 128 * n:128 * n + 128]
        scale = lax.rsqrt(jnp.sum(tot, axis=1, keepdims=True) * (1.0 / D) + EPS)
        rows = pl.ds(pl.multiple_of(k * 16, 16), 16)
        for m in range(4):
            cut = slice(1024 * m, 1024 * m + 1024)
            aexp[rows, cut] = (rows_of(cut) * scale * gffn[:, cut]).astype(BF16)
        return carry

    lax.fori_loop(0, NZ, expert_rows, 0)
    mark("s_expert")
    acc[...] = jnp.zeros_like(acc)

    def expert_in(k, carry):
        cut = pl.ds(pl.multiple_of(k * 512, 512), 512)
        lhs = aexp[:, cut]
        acc[:, 0:256] += dot(lhs, eg[cut, :])
        acc[:, 256:512] += dot(lhs, eu[cut, :])
        return carry

    lax.fori_loop(0, 8, expert_in, 0)
    g_ = acc[:, 0:256]
    hid = (g_ * jax.nn.sigmoid(g_) * acc[:, 256:512]).astype(BF16)
    aexp[:, 0:256] = hid

    mark("s3_hidden_stage")
    wait_for(halla.at[0, 0:3], lsem.at[0])
    wait_for(hallb.at[0, 0:3], lsem.at[1])
    for d in (2, 1, 3):
        px, py = lax.rem(ex_ + d, 4), lax.rem(ey + d, 4)
        rcopy(halla.at[ey], halla.at[ey], ssem.at[31], lsem.at[2], 4 * py + ex_, t).start()
        rcopy(hallb.at[ex_], hallb.at[ex_], ssem.at[32], lsem.at[3], 4 * ey + px, t).start()
    mark("s2_expert_out")

    def chunk_of(k):
        return lax.rem(k + e, 4)

    def expert_out(part_, k):
        at_ = pl.ds(pl.multiple_of(part_ * HALF + k * 512, 512), 512)
        return dot(aexp[:, 0:256], ed[:, at_])

    def for_mate(i, carry):
        k = chunk_of(i)
        prod = expert_out(1 - c, k).astype(BF16)
        for n in range(NZ):
            yp[k, n] = prod[16 * n:16 * n + 16]
        rcopy(yp.at[k], yd2d.at[k], ssem.at[15], dsem.at[k], e, mate).start()
        return carry

    def back(j, pe):
        rcopy(ys.at[1 - c, :, :, cols(j)], yin.at[:, e], ssem.at[18], rsem.at[12], pe, mate).start()

        @pl.when(pe != e)
        def _():
            rcopy(ys.at[c, :, :, cols(j)], yin.at[:, e], ssem.at[19], rsem.at[12], pe, t).start()

        @pl.when(pe == e)
        def _():
            yin[:, e] = ys[c, :, :, cols(j)]

    def for_own(i, carry):
        k = chunk_of(i)
        prod = expert_out(c, k)
        at_ = pl.ds(pl.multiple_of(k * 512, 512), 512)
        wait_for(yd2d.at[k], dsem.at[k])
        both_sum = jnp.concatenate([prod[16 * n:16 * n + 16] + yd2d[k, n].astype(F32) for n in range(NZ)], axis=0)
        compact = dot(keep_rows, both_sum.astype(BF16))
        for n in range(4):
            ys[n // 2, n % 2, :, at_] = compact[24 * n:24 * n + 24].astype(BF16)
        for j in range(2):
            back(2 * k + j, c * NZ + 2 * k + j)
        return carry

    lax.fori_loop(0, 4, for_mate, 0)
    lax.fori_loop(0, 4, for_own, 0)

    mark("t_wait_hidden")
    copies[19].wait()
    wait_for(halla.at[0:3], lsem.at[2])
    wait_for(hallb.at[0:3], lsem.at[3])
    wait_for(hallc.at[0:15], rsem.at[8])
    mark("u_down")

    def dense_down(g, carry):
        parts = (
            jnp.concatenate([hallc[4 * g + j] for j in range(4)], axis=0),
            jnp.concatenate([halla[g, j] for j in range(4)], axis=0),
            jnp.concatenate([hallb[j, g] for j in range(4)], axis=0),
        )
        prod = dot(jnp.concatenate(parts, axis=1), dd[...])
        for j in range(4):
            part2[2 * g + j // 2, j % 2] = prod[32 * j:32 * j + 32].astype(BF16)
        return carry

    lax.fori_loop(0, 4, dense_down, 0)
    rcopy(part2.at[:, 1 - c], pd2d2, ssem.at[16], rsem.at[10], e, mate).start()
    mark("v_wait_back")
    either(e // NZ == c, yin.at[:, 0:15], yin, rsem.at[12])
    wait_for(pd2d2, rsem.at[10])
    mark("w_combine")

    for g in range(2):
        rows = yin[g].astype(F32).reshape(384, COLS).astype(BF16)
        tot = dot(wtab[g, 0], rows) + dot(wtab[g, 1], rows)
        for m in range(4):
            k = 4 * g + m
            total_ = tot[32 * m:32 * m + 32] + part2[k, c].astype(F32) + pd2d2[k].astype(F32)
            rsend2[k] = total_.astype(BF16)
    over_z(lambda p: rcopy(rsend2.at[p], rrecv2.at[z], ssem.at[17], rsem.at[11], e, 2 * p + c).start())
    rrecv2[z] = rsend2[z]
    mark("x_wait_rs")
    wait_for(rrecv2.at[0:7], rsem.at[11])
    tot = resall[z, c].astype(F32)
    for k in range(NZ):
        tot = tot + rrecv2[k].astype(F32)
    outv[...] = tot.astype(BF16)

    mark("z_deliver")
    def deliver(d):
        p = lax.rem(z + d, NZ)

        @pl.when(jnp.logical_or(t != e, p != z))
        def _():
            rcopy(outv, ofull.at[:, cols(e)], ssem.at[20], osem.at[e], t, 2 * p + c).start()

    for d in Z_ORDER + (0,):
        deliver(d)

    @pl.when(t == e)
    def _():
        ofull[:, cols(e)] = outv[...]

    first = c == lax.rem(e, 2)

    @pl.when(first)
    def _():
        def pass_on(p):
            @pl.when(jnp.logical_or(t != e, p != e))
            def _():
                wait_for(ofull.at[:, cols(p)], osem.at[p])

            rcopy(ofull.at[:, cols(p)], ofull.at[:, cols(p)], ssem.at[22], rsem.at[14], e, mate).start()

        pass_on(e)
        for offset in EP_ORDER[::-1]:
            pass_on(behind(offset))
        wait_for(ofull, ssem.at[22])

    @pl.when(jnp.logical_not(first))
    def _():
        wait_for(ofull, rsem.at[14])

    mark("zz_end")
    wait_for(xall.at[0:15], ssem.at[0])
    wait_for(hallc.at[0:15], ssem.at[33])
    wait_for(rtall.at[0:15], ssem.at[1])
    wait_for(csend.at[0:15], ssem.at[2])
    wait_for(heads.at[:, 0:15 * HD], ssem.at[3])
    wait_for(mhall.at[0:15], ssem.at[23])
    wait_for(wp, ssem.at[4])
    wait_for(wpall.at[0:7 * HD], ssem.at[5])
    wait_for(resall.at[0, 0], ssem.at[6])
    wait_for(rsend2.at[0:7], ssem.at[7])
    wait_for(xsa.at[0:15], ssem.at[8])
    wait_for(xsb.at[0:15], ssem.at[27])
    wait_for(rsend2.at[0:7], ssem.at[9])
    wait_for(xfa.at[0:7, :, 0:HALF], ssem.at[10])
    wait_for(xfb.at[0:7, :, 0:HALF], ssem.at[28])
    for i, ref in ((11, dsg), (24, dsu), (25, d2g), (26, d2u)):
        wait_for(ref.at[0:3], ssem.at[i])
    wait_for(strecv.at[0:15], ssem.at[12])
    wait_for(xfa.at[0:7, :, 0:HALF], ssem.at[13])
    wait_for(xfb.at[0:7, :, 0:HALF], ssem.at[29])
    for i, ref in ((14, halla.at[0]), (30, hallb.at[0]), (31, halla), (32, hallb)):
        wait_for(ref.at[0:3], ssem.at[i])
    wait_for(yd2d, ssem.at[15])
    wait_for(pd2d2, ssem.at[16])
    wait_for(rsend2.at[0:7], ssem.at[17])
    wait_for(yin.at[:, 0:8], ssem.at[18])
    either(e // NZ == c, yin.at[:, 0:7], yin.at[:, 0:8], ssem.at[19])
    either(t == e, rsend2.at[0:7], rsend2, ssem.at[20])
    wait_for(wpall.at[0:7 * HD], ssem.at[21])
    mark(None)


def finish_kernel(out_v, nm_v, nn_v, nmax_v, out_o, nm_o, nn_o, nmax_o, sem):
    trips = [(nm_v.at[8 * k:8 * k + 8], nm_o.at[8 * k:8 * k + 8]) for k in range(4)]
    trips += [(out_v, out_o), (nn_v, nn_o), (nmax_v, nmax_o)]
    copies = [pltpu.make_async_copy(a, b, sem.at[i]) for i, (a, b) in enumerate(trips)]
    for copy in copies:
        copy.start()
    for copy in copies:
        copy.wait()


def on_device(
    tokens, state_matrix, state_norm, state_max, mixer_gain, w_query, w_key, w_value, w_outgate, w_ingate, w_forget,
    forget_bias, w_proj, ffn_gain, w_branch, routes, route_weight, expert_gate, expert_up, expert_down,
    dense_gate, dense_up, dense_down,
):
    any_ = pl.BlockSpec(memory_space=pltpu.HBM)
    local = pl.BlockSpec(memory_space=pltpu.VMEM)
    vm = pltpu.VMEM
    scratch = [
        vm((ROWS, D), BF16), vm((ROWS, HD, HD), F32), vm((ROWS, HD), F32), vm((1, ROWS), F32), vm((1, D), F32),
        vm((COLS, 512), BF16), vm((N, D), BF16), vm((N, D), BF16), vm((1, N), F32), vm((HD, COLS), BF16),
        vm((1, D), F32), vm((ROWS, HD), BF16), vm((2, ROWS), jnp.int32), vm((2, ROWS), F32),
        vm((D, COLS), BF16), vm((D, COLS), BF16), vm((COLS, D), BF16), vm((COLS, 1024), BF16), vm((512, COLS), BF16),
        vm((N, ROWS, COLS), BF16), vm((N, ROWS, 512), BF16), vm((N, ROWS, 512), BF16), vm((N, ROWS, HD), BF16),
        vm((ROWS, HALF), BF16), vm((ROWS, HD), F32),
        vm((HALF, COLS), BF16), vm((2, 2, 128, 384), BF16), vm((NZ, 2, ROWS, COLS), BF16),
        vm((NZ, 2, ROWS, COLS), BF16), vm((NZ, ROWS, COLS), BF16), vm((NZ, ROWS, COLS), BF16),
        vm((NZ, ROWS, COLS), BF16),
        vm((8, 128), F32), vm((N, 8, 128), F32),
        vm((4, 4, ROWS, 512), BF16), vm((4, 4, ROWS, 512), BF16), vm((4, 4, ROWS, 512), BF16),
        vm((4, 4, ROWS, 512), BF16), vm((4, ROWS, 512), BF16), vm((4, ROWS, 512), BF16), vm((4, ROWS, 512), BF16),
        vm((4, ROWS, 512), BF16),
        vm((4, 8, 128), F32), vm((N, 8, 128), F32), vm((4, 4, ROWS, HD), BF16),
        vm((4, 4, ROWS, HD), BF16), vm((N, ROWS, COLS), BF16), vm((512, COLS), BF16),
        vm((512, COLS), BF16),
        vm((N, 8, COLS), BF16), vm((N, 4, COLS), BF16), vm((NZ, 8, D), BF16), vm((NZ, 4, D), BF16), vm((128, D), BF16), vm((128, 512), F32),
        vm((4, NZ, 16, 512), BF16), vm((4, NZ, 16, 512), BF16), vm((2, 2, 24, HALF), BF16), vm((2, N, 24, COLS), BF16),
        vm((ROWS, COLS), BF16),
        pltpu.SemaphoreType.DMA((23,)), pltpu.SemaphoreType.DMA((34,)), pltpu.SemaphoreType.DMA((N,)),
        pltpu.SemaphoreType.DMA((16,)), pltpu.SemaphoreType.DMA((4, NZ)), pltpu.SemaphoreType.DMA((4, NZ)),
        pltpu.SemaphoreType.DMA((N,)), pltpu.SemaphoreType.DMA((N,)), pltpu.SemaphoreType.DMA((4,)),
        pltpu.SemaphoreType.DMA((4,)), pltpu.SemaphoreType.DMA((4,)),
    ]
    results = pl.pallas_call(
        layer_kernel,
        out_shape=(vm((ROWS, D), BF16), vm((ROWS, HD, HD), F32), vm((ROWS, HD), F32), vm((1, ROWS), F32)),
        in_specs=[any_] * 23,
        out_specs=(local,) * 4,
        scratch_shapes=scratch,
        compiler_params=pltpu.CompilerParams(
            collective_id=0, has_side_effects=True, vmem_limit_bytes=60 * 1024 * 1024
        ),
        name="layer",
    )(
        tokens, state_matrix.reshape(ROWS, HD, HD), state_norm.reshape(ROWS, HD), state_max.T,
        mixer_gain.reshape(1, D), w_query, w_key, w_value, w_outgate, w_ingate.T, w_forget.T,
        forget_bias.reshape(1, N), w_proj, ffn_gain.reshape(1, D), w_branch.reshape(ROWS, HD), routes.T,
        route_weight.T, expert_gate, expert_up, expert_down, dense_gate, dense_up, dense_down,
    )
    out, nm, nn, nmax = pl.pallas_call(
        finish_kernel,
        out_shape=(
            jax.ShapeDtypeStruct((ROWS, D), BF16), jax.ShapeDtypeStruct((ROWS, HD, HD), F32),
            jax.ShapeDtypeStruct((ROWS, HD), F32), jax.ShapeDtypeStruct((1, ROWS), F32),
        ),
        in_specs=[local] * 4,
        out_specs=(any_,) * 4,
        scratch_shapes=[pltpu.SemaphoreType.DMA((7,))],
        compiler_params=pltpu.CompilerParams(vmem_limit_bytes=8 * 1024 * 1024),
        name="finish",
    )(*results)
    return (
        out, nm.reshape(ROWS, 1, HD, HD), nn.reshape(ROWS, 1, HD), nmax.T,
    )


def solution(mesh):
    in_specs = (
        P("ep", None), P("ep", "tp", None, None), P("ep", "tp", None), P("ep", "tp"), P(),
        P("ep", "tp"), P("ep", "tp"), P("ep", "tp"), P("ep", "tp"), P(), P(), P(), P("tp", "ep"), P(), P(),
        P("ep", None), P("ep", None), P("ep", None, "tp"), P("ep", None, "tp"), P("ep", "tp", None),
        P("ep", "tp"), P("ep", "tp"), P("tp", "ep"),
    )
    out_specs = (P("ep", None), P("ep", "tp", None, None), P("ep", "tp", None), P("ep", "tp"))
    return jax.shard_map(on_device, mesh=mesh, in_specs=in_specs, out_specs=out_specs, check_vma=False)
```
